32 devices in a mesh: sp: 8 (over z, x), tp: 4 (over y, core).
Axes of the slice: x: 2, y: 2, z: 4, core: 2. Of those that a mesh axis runs over, the one named last changes fastest.
Arguments:
- tokens: bfloat16 [1024, 2048], P(('sp', 'tp')), may hold values from -6 to 6
- conv_input: bfloat16 [2048, 512], P(None, 'tp'), may hold values from -0.125 to 0.125
- conv_gate: bfloat16 [2048, 512], P(None, 'tp'), may hold values from -0.125 to 0.125
- query_weight: bfloat16 [2048, 1024], P(None, 'tp'), may hold values from -0.125 to 0.125
- key_weight: bfloat16 [2048, 512], P(None, 'tp'), may hold values from -0.125 to 0.125
- value_weight: bfloat16 [2048, 512], P(None, 'tp'), may hold values from -0.125 to 0.125
- conv_taps: float32 [31, 512], P(None, 'tp'), may hold values from -4.5 to 4.5
- conv_gain: float32 [512], P('tp'), may hold values from 0.1 to 1.9
- key_offsets: bfloat16 [1024, 8], P('sp', 'tp'), may hold values from -16 to 2
- stick_gain: float32 [1024], P('tp'), may hold values from 0.1 to 1.9
- conv_output: bfloat16 [512, 2048], P('tp'), may hold values from -0.15625 to 0.15625
- stick_output: bfloat16 [1024, 2048], P('tp'), may hold values from -0.15625 to 0.15625
Outputs:
- mixed: bfloat16 [1024, 2048], P(('sp', 'tp'))
The draws below stay inside these ranges and needn't reach their ends.
All inputs are finite; a program needn't handle non-finite values.
Results may differ from the reference program's by a relative error of at most 0.013.
Values may be sent and summed in bfloat16 or wider, within the bound.
No kernel may reach another device: no remote copies, remote signals or barrier semaphores. Data moves between devices by JAX's collectives and lax.ppermute only.
A program may use at most 64 MiB of HBM per device.

```python
import jax
import jax.numpy as jnp
from jax import lax

D = 2048
CONV_CH = 512
HEAD_DIM = 128
STICK_HEADS = 8
KV_HEADS = 4
CONV_WIDTH = 31
TOK_DEV = 128
SEQUENCE_TOKENS = 1024
N_TP = 4


def draw_key_offsets(key, part):
    flow_lanes = jax.random.split(jax.random.fold_in(key, 11), 4)
    head_order = jax.random.permutation(flow_lanes[0], STICK_HEADS)
    slow_heads = (head_order < STICK_HEADS // 2).astype(jnp.float32)
    slow_level = -jnp.log(jnp.float32(SEQUENCE_TOKENS)) - 0.8
    ground_level = slow_heads * slow_level + (1.0 - slow_heads) * -4.2
    block_displacement = jax.random.uniform(flow_lanes[1], (SEQUENCE_TOKENS // TOK_DEV, 1, STICK_HEADS), jnp.float32, -0.7, 0.7)
    block_displacement = jnp.broadcast_to(block_displacement, (SEQUENCE_TOKENS // TOK_DEV, TOK_DEV, STICK_HEADS)).reshape(SEQUENCE_TOKENS, STICK_HEADS)
    random_wiggle = 0.4 * jnp.clip(jax.random.normal(flow_lanes[2], (SEQUENCE_TOKENS, STICK_HEADS), jnp.float32), -3.0, 3.0)
    spurt_rows = jax.random.randint(flow_lanes[3], (1, 10, STICK_HEADS), 0, SEQUENCE_TOKENS)
    position_list = jnp.arange(SEQUENCE_TOKENS, dtype=jnp.int32)[:, None, None]
    spurts_list = jnp.any(position_list == spurt_rows, axis=1)
    offset_list = jnp.where(spurts_list, block_displacement + random_wiggle, ground_level + block_displacement + random_wiggle)
    return offset_list.astype(jnp.bfloat16)


def draw_conv_taps(key, part):
    flow_lanes = jax.random.split(jax.random.fold_in(key, 23), 2)
    rise = jnp.exp(jnp.log(4.0) * jnp.arange(CONV_CH, dtype=jnp.float32) / CONV_CH)
    wobble = jnp.exp(jax.random.uniform(flow_lanes[1], (CONV_CH,), jnp.float32, -0.35, 0.35))
    rough = jnp.clip(jax.random.normal(flow_lanes[0], (CONV_WIDTH, CONV_CH), jnp.float32), -4.0, 4.0)
    return jnp.clip(rough * rise * wobble * CONV_WIDTH ** (-0.5), -4.5, 4.5)


def shard_levels(rng, shape, shards, least, top_value):
    def one(dim, shards_of):
        draws = jax.random.uniform(jax.random.fold_in(jax.random.fold_in(rng, 6), dim), (shards_of,), jnp.float32, least / len(shards), top_value / len(shards))
        return jnp.repeat(jnp.exp(draws), shape[dim] // shards_of).reshape((-1,) + (1,) * (len(shape) - dim - 1))

    factor_of = one(*shards[0])
    for cut in shards[1:]:
        factor_of = factor_of * one(*cut)
    return factor_of


def gaussian(rng, shape, width, reach, cuts=(), held_as=jnp.bfloat16):
    gain = shard_levels(rng, shape, cuts, -0.22, 0.18) if cuts else 1.0
    array = jax.random.normal(rng, shape, jnp.float32) * width * gain
    return jnp.minimum(jnp.maximum(array, -reach), reach).astype(held_as)


def setup_inputs(seed: int = 0) -> dict:
    arg_keys = jax.random.split(jax.random.key(seed), 13)
    tokens = gaussian(arg_keys[0], (SEQUENCE_TOKENS, D), 1.0, 6.0, ((0, 32),))
    conv_input = gaussian(arg_keys[1], (D, CONV_CH), D ** -0.5, 0.125, ((1, 4),))
    conv_gate = gaussian(arg_keys[2], (D, CONV_CH), D ** -0.5, 0.125, ((1, 4),))
    query_weight = gaussian(arg_keys[3], (D, STICK_HEADS * HEAD_DIM), D ** -0.5, 0.125, ((1, 4),))
    key_weight = gaussian(arg_keys[4], (D, KV_HEADS * HEAD_DIM), D ** -0.5, 0.125, ((1, 4),))
    value_weight = gaussian(arg_keys[5], (D, KV_HEADS * HEAD_DIM), D ** -0.5, 0.125, ((1, 4),))
    conv_taps = draw_conv_taps(jax.random.fold_in(arg_keys[12], 71), 0)
    conv_gain = jnp.clip(1.0 + 0.18 * jax.random.normal(arg_keys[7], (CONV_CH,), jnp.float32), 0.1, 1.9)
    key_offsets = draw_key_offsets(jax.random.fold_in(arg_keys[12], 71), 0)
    stick_gain = jnp.clip(1.0 + 0.18 * jax.random.normal(arg_keys[9], (STICK_HEADS * HEAD_DIM,), jnp.float32), 0.1, 1.9)
    conv_output = gaussian(arg_keys[10], (CONV_CH, D), (CONV_CH + STICK_HEADS * HEAD_DIM) ** -0.5, 0.15625, ((0, 4),))
    stick_output = gaussian(arg_keys[11], (STICK_HEADS * HEAD_DIM, D), (CONV_CH + STICK_HEADS * HEAD_DIM) ** -0.5, 0.15625, ((0, 4),))
    return dict(tokens=tokens, conv_input=conv_input, conv_gate=conv_gate, query_weight=query_weight, key_weight=key_weight, value_weight=value_weight, conv_taps=conv_taps, conv_gain=conv_gain, key_offsets=key_offsets, stick_gain=stick_gain, conv_output=conv_output, stick_output=stick_output)


norm_eps = 1e-05

def stick_head(queries, key_rows, values, offset_list):
    block_count = SEQUENCE_TOKENS // TOK_DEV
    score_scale = HEAD_DIM ** (-0.5)
    position_list = lax.iota(jnp.int32, TOK_DEV)

    def one_block(block_no):
        query_block = lax.dynamic_slice_in_dim(queries, block_no * TOK_DEV, TOK_DEV, 0)
        query_pos = block_no * TOK_DEV + position_list

        def walk_step(turn_no, carried):
            output, log_carry = carried
            start_row = (block_no - turn_no) * TOK_DEV
            key_part = lax.dynamic_slice_in_dim(key_rows, start_row, TOK_DEV, 0)
            value_part = lax.dynamic_slice_in_dim(values, start_row, TOK_DEV, 0)
            offset_part = lax.dynamic_slice_in_dim(offset_list, start_row, TOK_DEV, 0)
            scores = jnp.dot(query_block, key_part.T, preferred_element_type=jnp.float32) * score_scale
            scores = scores + offset_part[None, :]
            allowed = (start_row + position_list)[None, :] < query_pos[:, None]
            log_keep = jnp.where(allowed, jax.nn.log_sigmoid(-scores), 0.0)
            after = lax.cumsum(log_keep, axis=1, reverse=True) - log_keep
            weights = jnp.where(allowed, jnp.exp(jax.nn.log_sigmoid(scores) + after + log_carry), 0.0)
            weights = weights.astype(jnp.bfloat16)
            output = output + jnp.dot(weights, value_part, preferred_element_type=jnp.float32)
            log_carry = log_carry + lax.optimization_barrier(jnp.sum(log_keep, axis=1, keepdims=True))
            return (output, log_carry)
        start_state = (jnp.zeros((TOK_DEV, HEAD_DIM), jnp.float32), jnp.zeros((TOK_DEV, 1), jnp.float32))
        output, log_carry = lax.fori_loop(0, block_no + 1, walk_step, start_state)
        return output
    blocks = lax.map(one_block, jnp.arange(block_count, dtype=jnp.int32))
    return blocks.reshape(SEQUENCE_TOKENS, HEAD_DIM)

def reference(tokens, conv_input, conv_gate, query_weight, key_weight, value_weight, conv_taps, conv_gain, key_offsets, stick_gain, conv_output, stick_output):
    conv_values = jnp.dot(tokens, conv_input, preferred_element_type=jnp.float32).astype(jnp.bfloat16)
    conv_gates = jnp.dot(tokens, conv_gate, preferred_element_type=jnp.float32).astype(jnp.bfloat16)
    blended = (conv_values.astype(jnp.float32) * jax.nn.sigmoid(conv_gates.astype(jnp.float32))).astype(jnp.bfloat16)
    reach_rows = CONV_WIDTH - 1
    widened = jnp.concatenate([jnp.zeros((reach_rows, CONV_CH), jnp.float32), blended.astype(jnp.float32)], axis=0)
    conv_field = conv_taps[0] * widened[0:SEQUENCE_TOKENS]
    for tap_index in range(1, CONV_WIDTH):
        conv_field = conv_field + conv_taps[tap_index] * widened[tap_index:tap_index + SEQUENCE_TOKENS]
    center = lax.optimization_barrier(jnp.mean(conv_field, axis=1, keepdims=True))
    spread = lax.optimization_barrier(jnp.mean(jnp.square(conv_field - center), axis=1, keepdims=True))
    conv_mix = jax.nn.silu((conv_field - center) * lax.rsqrt(spread + norm_eps) * conv_gain).astype(jnp.bfloat16)
    queries = jnp.dot(tokens, query_weight, preferred_element_type=jnp.float32).astype(jnp.bfloat16)
    key_rows = jnp.dot(tokens, key_weight, preferred_element_type=jnp.float32).astype(jnp.bfloat16)
    values = jnp.dot(tokens, value_weight, preferred_element_type=jnp.float32).astype(jnp.bfloat16)
    per_group = STICK_HEADS // KV_HEADS

    def one_head(head_no):
        kv_no = head_no // per_group
        query_head = lax.dynamic_slice_in_dim(queries, head_no * HEAD_DIM, HEAD_DIM, 1)
        key_head = lax.dynamic_slice_in_dim(key_rows, kv_no * HEAD_DIM, HEAD_DIM, 1)
        value_head = lax.dynamic_slice_in_dim(values, kv_no * HEAD_DIM, HEAD_DIM, 1)
        offset_head = lax.dynamic_index_in_dim(key_offsets, head_no, 1, keepdims=False).astype(jnp.float32)
        return stick_head(query_head, key_head, value_head, offset_head)
    attended = lax.map(one_head, jnp.arange(STICK_HEADS, dtype=jnp.int32))
    mean_square = lax.optimization_barrier(jnp.mean(attended * attended, axis=2, keepdims=True))
    normed = attended * lax.rsqrt(mean_square + norm_eps)
    stick_mix = (jnp.transpose(normed, (1, 0, 2)).reshape(SEQUENCE_TOKENS, STICK_HEADS * HEAD_DIM) * stick_gain).astype(jnp.bfloat16)
    conv_share = CONV_CH // N_TP
    stick_share = STICK_HEADS * HEAD_DIM // N_TP
    summed = jnp.zeros((SEQUENCE_TOKENS, D), jnp.float32)
    for member in range(N_TP):
        conv_cols = slice(member * conv_share, (member + 1) * conv_share)
        stick_cols = slice(member * stick_share, (member + 1) * stick_share)
        partial_sum = jnp.dot(conv_mix[:, conv_cols], conv_output[conv_cols], preferred_element_type=jnp.float32)
        partial_sum = partial_sum + jnp.dot(stick_mix[:, stick_cols], stick_output[stick_cols], preferred_element_type=jnp.float32)
        rounded = lax.optimization_barrier(partial_sum.astype(jnp.bfloat16))
        summed = summed + rounded.astype(jnp.float32)
    return summed.astype(jnp.bfloat16)
```

```python
import functools

import jax
import jax.numpy as jnp
from jax import lax
from jax.experimental import pallas as pl
from jax.experimental.pallas import tpu as pltpu
from jax.sharding import PartitionSpec as P

HEAD_DIM = 128
norm_eps = 1e-05
f32 = jnp.float32
bf16 = jnp.bfloat16


def swap(value, axis, by):
    count = lax.axis_size(axis)
    return lax.ppermute(value, axis, [(i, i ^ by) for i in range(count)])


def from_behind(value, axis, by):
    count = lax.axis_size(axis)
    pairs = [(i, i + by) for i in range(count) if 0 <= i + by < count]
    return lax.ppermute(value, axis, pairs)


def dot(a, b):
    return jnp.dot(a, b, preferred_element_type=f32)


def project_kernel(*refs, pieces):
    toks = refs[:pieces]
    w_in, w_gate, w_q, w_k, w_v, off, pay, qs, blend, tail, x_all = refs[pieces:]
    rows = toks[0].shape[0]
    me = lax.axis_index("tp")
    for k in range(pieces):
        x_all[pl.ds(pl.multiple_of((me ^ k) * rows, rows), rows), :] = toks[k][...]
    x = x_all[...]
    n = x.shape[0]
    kv = w_k.shape[1]
    pay[0:n, 0:kv] = dot(x, w_k[...]).astype(bf16)
    pay[0:n, kv : 2 * kv] = dot(x, w_v[...]).astype(bf16)
    pay[n:, 0:kv] = off[...]
    pay[n:, kv : 2 * kv] = jnp.zeros_like(off)
    q = dot(x, w_q[...]).astype(bf16)
    for h in range(q.shape[1] // HEAD_DIM):
        qs[h * n : (h + 1) * n, :] = q[:, h * HEAD_DIM : (h + 1) * HEAD_DIM]
    values = dot(x, w_in[...]).astype(bf16).astype(f32)
    gates = dot(x, w_gate[...]).astype(bf16).astype(f32)
    b = (values * jax.nn.sigmoid(gates)).astype(bf16)
    blend[...] = b
    tail[...] = b[n - tail.shape[0] :, :]


def conv_kernel(halo, blend, taps, field, stats, wide):
    n = blend.shape[0]
    h = halo.shape[0]
    reach = taps.shape[0] - 1
    wide[0:h, :] = halo[...].astype(f32)
    wide[h : h + n, :] = blend[...].astype(f32)
    base = h - reach
    f = taps[0:1, :] * wide[base : base + n, :]
    for t in range(1, reach + 1):
        f = f + taps[t : t + 1, :] * wide[base + t : base + t + n, :]
    field[...] = f
    ch = f.shape[1]
    mean = jnp.sum(f, axis=1, keepdims=True) / ch
    d = f - mean
    m2 = jnp.sum(d * d, axis=1, keepdims=True)
    stats[0:1, :] = jnp.transpose(jnp.broadcast_to(mean, (n, 128)))[0:1, :]
    stats[1:2, :] = jnp.transpose(jnp.broadcast_to(m2, (n, 128)))[0:1, :]


def block_part(q, pay, gap, n, per, tri):
    kv = HEAD_DIM
    keys = pay[0:n, 0:kv]
    vals = pay[0:n, kv : 2 * kv]
    off = pay[n : n + 8, 0:kv].astype(f32)
    s = lax.dot_general(q, keys, (((1,), (1,)), ((), ())), preferred_element_type=f32)
    s = s * (HEAD_DIM ** (-0.5))
    shift = jnp.concatenate(
        [jnp.broadcast_to(off[h : h + 1, :], (n, n)) for h in range(per)], axis=0
    )
    s = s + shift
    row = lax.broadcasted_iota(jnp.int32, s.shape, 0) & (n - 1)
    col = lax.broadcasted_iota(jnp.int32, s.shape, 1)
    allowed = col < row + gap
    soft = jnp.log1p(jnp.exp(-jnp.abs(s)))
    take = jnp.minimum(s, 0.0) - soft
    keep = jnp.where(allowed, jnp.minimum(-s, 0.0) - soft, 0.0)
    hi = keep.astype(bf16)
    lo = (keep - hi.astype(f32)).astype(bf16)
    sums = dot(hi, tri) + dot(lo, tri)
    w = jnp.where(allowed, jnp.exp(take + sums[:, 0:n]), 0.0).astype(bf16)
    return dot(w, vals), sums[:, n : 2 * n]


def tri_of(n):
    r = lax.broadcasted_iota(jnp.int32, (n, 2 * n), 0)
    c = lax.broadcasted_iota(jnp.int32, (n, 2 * n), 1)
    return jnp.where((r > c) | (c >= n), 1.0, 0.0).astype(bf16)


def finish(att, field, stats, c_gain, s_gain, w_c, w_s, mine, other, send, mix, n, per, members):
    ch = field.shape[1]
    mean = sum(st[0:1, :] for st in stats) / members
    m2 = sum(st[1:2, :] for st in stats)
    m2 = m2 + ch * sum((st[0:1, :] - mean) ** 2 for st in stats)
    rstd = lax.rsqrt(m2 / (ch * members) + norm_eps)
    mean_c = jnp.transpose(jnp.broadcast_to(mean, (ch, n)))
    rstd_c = jnp.transpose(jnp.broadcast_to(rstd, (ch, n)))
    z = (field[...] - mean_c) * rstd_c * c_gain[...]
    mix[:, 0:ch] = (z * jax.nn.sigmoid(z)).astype(bf16)
    ms = jnp.mean(att * att, axis=1, keepdims=True)
    normed = att * lax.rsqrt(ms + norm_eps)
    for h in range(per):
        part = normed[h * n : (h + 1) * n, :] * s_gain[h : h + 1, :]
        mix[:, ch + h * HEAD_DIM : ch + (h + 1) * HEAD_DIM] = part.astype(bf16)
    me = lax.axis_index("tp")
    rows = n // members
    lhs = jnp.concatenate(
        [mix[pl.ds(pl.multiple_of((me ^ k) * rows, rows), rows), :] for k in (0, 2, 1, 3)], axis=0
    )
    out = dot(lhs[:, 0:ch], w_c[...]) + dot(lhs[:, ch:], w_s[...])
    mine[...] = out[0:rows, :]
    other[...] = out[rows : 2 * rows, :]
    send[...] = out[2 * rows :, :].astype(bf16)


def attend_kernel(*refs, blocks, members, n, per):
    q_ref = refs[0]
    pays = refs[1 : 1 + blocks]
    field = refs[1 + blocks]
    stats = refs[2 + blocks : 2 + blocks + members]
    c_gain, s_gain, w_c, w_s, mine, other, send, mix, parts, totals = refs[2 + blocks + members :]
    me = lax.axis_index("sp")
    q = q_ref[...]
    tri = tri_of(n)
    for k in range(blocks):
        j = me ^ k
        part, total = block_part(q, pays[k], (me - j) * n, n, per, tri)
        parts[pl.ds(j, 1)] = part[None]
        totals[pl.ds(j, 1)] = total[None]
    att = parts[blocks - 1]
    carry = totals[blocks - 1]
    for j in range(blocks - 2, -1, -1):
        att = att + jnp.exp(carry) * parts[j]
        if j:
            carry = carry + totals[j]
    finish(att, field, stats, c_gain, s_gain, w_c, w_s, mine, other, send, mix, n, per, members)


def attend_loop_kernel(*refs, members, n, per):
    q_ref, pays, field = refs[:3]
    stats = refs[3 : 3 + members]
    c_gain, s_gain, w_c, w_s, mine, other, send, mix = refs[3 + members :]
    me = lax.axis_index("sp")
    q = q_ref[...]
    tri = tri_of(n)

    def step(turn, carried):
        att, carry = carried
        j = me - turn
        part, total = block_part(q, pays.at[j], turn * n, n, per, tri)
        return att + jnp.exp(carry) * part, carry + total

    zero = jnp.zeros((per * n, HEAD_DIM), f32)
    att, _ = lax.fori_loop(0, me + 1, step, (zero, zero))
    finish(att, field, stats, c_gain, s_gain, w_c, w_s, mine, other, send, mix, n, per, members)


def call(body, outs, *args, scratch=(), flops=0):
    spec = pl.BlockSpec(memory_space=pltpu.VMEM)
    return pl.pallas_call(
        body,
        out_shape=outs,
        in_specs=[spec] * len(args),
        out_specs=[spec] * len(outs),
        scratch_shapes=scratch,
        cost_estimate=pl.CostEstimate(flops=flops, transcendentals=0, bytes_accessed=0),
    )(*args)


def shards(
    tokens,
    conv_input,
    conv_gate,
    query_weight,
    key_weight,
    value_weight,
    conv_taps,
    conv_gain,
    key_offsets,
    stick_gain,
    conv_output,
    stick_output,
):
    members = lax.axis_size("tp")
    blocks = lax.axis_size("sp")
    rows, width = tokens.shape
    n = rows * members
    ch = conv_input.shape[1]
    kv = key_weight.shape[1]
    per = query_weight.shape[1] // kv
    off = jnp.pad(jnp.transpose(key_offsets), ((0, 8 - per), (0, 0)))
    by_core = swap(tokens, "tp", 1)
    by_chip = swap(tokens, "tp", 2)
    by_both = swap(by_chip, "tp", 1)
    pay, qs, blend, tail = call(
        functools.partial(project_kernel, pieces=4),
        [
            jax.ShapeDtypeStruct((n + 8, 2 * kv), bf16),
            jax.ShapeDtypeStruct((per * n, HEAD_DIM), bf16),
            jax.ShapeDtypeStruct((n, ch), bf16),
            jax.ShapeDtypeStruct((32, ch), bf16),
        ],
        tokens, by_core, by_chip, by_both,
        conv_input, conv_gate, query_weight, key_weight, value_weight, off,
        scratch=[pltpu.VMEM((n, width), bf16)],
        flops=2 * n * width * (2 * ch + 4 * kv),
    )
    halo = from_behind(tail, "sp", 1)
    if blocks == 8:
        z6 = swap(pay, "sp", 6)
        z4 = swap(pay, "sp", 4)
        z2 = swap(pay, "sp", 2)
        x1 = swap(pay, "sp", 1)
        pays = [pay, x1, z2, swap(z2, "sp", 1), z4, swap(z4, "sp", 1), z6, swap(z6, "sp", 1)]
    else:
        pays = [lax.all_gather(pay, "sp", axis=0)]
    field, stats = call(
        conv_kernel,
        [jax.ShapeDtypeStruct((n, ch), f32), jax.ShapeDtypeStruct((8, n), f32)],
        halo, blend, conv_taps,
        scratch=[pltpu.VMEM((n + 32, ch), f32)],
        flops=64 * n * ch,
    )
    stats_chip = swap(stats, "tp", 2)
    all_stats = [stats, swap(stats, "tp", 1), stats_chip, swap(stats_chip, "tp", 1)]
    scratch = [pltpu.VMEM((n, ch + per * HEAD_DIM), bf16)]
    if blocks == 8:
        body = functools.partial(attend_kernel, blocks=blocks, members=members, n=n, per=per)
        scratch += [pltpu.VMEM((blocks, per * n, HEAD_DIM), f32)] * 2
    else:
        body = functools.partial(attend_loop_kernel, members=members, n=n, per=per)
    mine, other, send = call(
        body,
        [
            jax.ShapeDtypeStruct((rows, width), f32),
            jax.ShapeDtypeStruct((rows, width), f32),
            jax.ShapeDtypeStruct((2 * rows, width), bf16),
        ],
        qs, *pays, field, *all_stats,
        conv_gain.reshape(1, ch), stick_gain.reshape(per, HEAD_DIM), conv_output, stick_output,
        scratch=scratch,
        flops=2 * n * width * (ch + per * HEAD_DIM),
    )
    got = swap(send, "tp", 1).astype(f32)
    chip = swap((other + got[rows:]).astype(bf16), "tp", 2)
    return (mine + got[:rows] + chip.astype(f32)).astype(bf16)


def solution(mesh):
    return jax.shard_map(
        shards,
        mesh=mesh,
        in_specs=(
            P(("sp", "tp"), None),
            P(None, "tp"),
            P(None, "tp"),
            P(None, "tp"),
            P(None, "tp"),
            P(None, "tp"),
            P(None, "tp"),
            P("tp"),
            P("sp", "tp"),
            P("tp"),
            P("tp", None),
            P("tp", None),
        ),
        out_specs=P(("sp", "tp"), None),
        check_vma=False,
    )
```

```python
import functools

import jax
import jax.numpy as jnp
from jax import lax
from jax.experimental import pallas as pl
from jax.experimental.pallas import tpu as pltpu
from jax.sharding import PartitionSpec as P

HEAD_DIM = 128
norm_eps = 1e-05
f32 = jnp.float32
bf16 = jnp.bfloat16


def swap(value, axis, by):
    count = lax.axis_size(axis)
    return lax.ppermute(value, axis, [(i, i ^ by) for i in range(count)])


def from_behind(value, axis, by):
    count = lax.axis_size(axis)
    pairs = [(i, i + by) for i in range(count) if 0 <= i + by < count]
    return lax.ppermute(value, axis, pairs)


def dot(a, b):
    return jnp.dot(a, b, preferred_element_type=f32)


def load_kernel(*refs):
    sources, sems = refs[:12], refs[-1]
    tokens, w_in, w_gate, w_q, w_k, w_v, taps, c_gain, off, s_gain, w_c, w_s = sources
    tok, conv_w, q_w, kv_w, taps_v, c_gain_v, off_v, s_gain_v, out_w = refs[12:-1]
    ch = w_in.shape[1]
    kv = w_k.shape[1]
    pairs = [
        (w_k, kv_w.at[:, 0:kv]),
        (w_v, kv_w.at[:, kv:]),
        (w_q, q_w),
        (w_in, conv_w.at[:, 0:ch]),
        (w_gate, conv_w.at[:, ch:]),
        (tokens, tok),
        (taps, taps_v),
        (c_gain, c_gain_v),
        (off, off_v),
        (s_gain, s_gain_v),
        (w_c, out_w.at[0:ch]),
        (w_s, out_w.at[ch:]),
    ]
    copies = [pltpu.make_async_copy(a, b, sems.at[i]) for i, (a, b) in enumerate(pairs)]
    for copy in copies:
        copy.start()
    for copy in copies:
        copy.wait()


def project_kernel(t0, t1, t2, t3, conv_w, q_w, kv_w, off, pay, qs, blend, x_all):
    rows = t0.shape[0]
    me = lax.axis_index("tp")
    for k, t in enumerate((t0, t1, t2, t3)):
        x_all[pl.ds(pl.multiple_of((me ^ k) * rows, rows), rows), :] = t[...]
    x = x_all[...]
    n = x.shape[0]
    ch = conv_w.shape[1] // 2
    kv = kv_w.shape[1] // 2
    pay[0:n, :] = dot(x, kv_w[...]).astype(bf16)
    q = dot(x, q_w[...]).astype(bf16)
    for h in range(q.shape[1] // HEAD_DIM):
        qs[h * n : (h + 1) * n, :] = q[:, h * HEAD_DIM : (h + 1) * HEAD_DIM]
    both = dot(x, conv_w[...]).astype(bf16).astype(f32)
    b = (both[:, 0:ch] * jax.nn.sigmoid(both[:, ch:])).astype(bf16)
    blend[...] = b
    row = lax.broadcasted_iota(jnp.int32, (16, kv), 0)
    pay[n:, 0:kv] = jnp.where(row < 2, off[...], b[n - 32 : n - 16, :])
    pay[n:, kv:] = b[n - 16 :, :]


def conv_kernel(p1, p3, p7, blend, taps, field, stats, wide):
    n = blend.shape[0]
    half = p1.shape[1] // 2
    reach = taps.shape[0] - 1
    me = lax.axis_index("sp")
    flip = me ^ (me - 1)
    halo = jnp.where(flip == 1, p1[n:, :], jnp.where(flip == 3, p3[n:, :], p7[n:, :]))
    halo = jnp.where(me > 0, halo.astype(f32), 0.0)
    wide[0:16, :] = halo[:, 0:half]
    wide[16:32, :] = halo[:, half:]
    convolve(blend, taps, field, stats, wide)


def conv_plain_kernel(halo, blend, taps, field, stats, wide):
    wide[0:32, :] = halo[...].astype(f32)
    convolve(blend, taps, field, stats, wide)


def convolve(blend, taps, field, stats, wide):
    n = blend.shape[0]
    reach = taps.shape[0] - 1
    wide[32 : 32 + n, :] = blend[...].astype(f32)
    base = 32 - reach
    f = taps[0:1, :] * wide[base : base + n, :]
    for t in range(1, reach + 1):
        f = f + taps[t : t + 1, :] * wide[base + t : base + t + n, :]
    field[...] = f
    ch = f.shape[1]
    mean = jnp.sum(f, axis=1, keepdims=True) / ch
    d = f - mean
    m2 = jnp.sum(d * d, axis=1, keepdims=True)
    stats[0:1, :] = jnp.transpose(jnp.broadcast_to(mean, (n, 128)))[0:1, :]
    stats[1:2, :] = jnp.transpose(jnp.broadcast_to(m2, (n, 128)))[0:1, :]


def block_part(q, pay, gap, n, per, tri):
    kv = HEAD_DIM
    keys = pay[0:n, 0:kv]
    vals = pay[0:n, kv : 2 * kv]
    off = pay[n : n + 16, 0:kv].astype(f32)
    s = lax.dot_general(q, keys, (((1,), (1,)), ((), ())), preferred_element_type=f32)
    s = s * (HEAD_DIM ** (-0.5))
    shift = jnp.concatenate(
        [jnp.broadcast_to(off[h : h + 1, :], (n, n)) for h in range(per)], axis=0
    )
    s = s + shift
    row = lax.broadcasted_iota(jnp.int32, s.shape, 0) & (n - 1)
    col = lax.broadcasted_iota(jnp.int32, s.shape, 1)
    allowed = col < row + gap
    soft = jnp.log1p(jnp.exp(-jnp.abs(s)))
    take = jnp.minimum(s, 0.0) - soft
    keep = jnp.where(allowed, jnp.minimum(-s, 0.0) - soft, 0.0)
    hi = keep.astype(bf16)
    lo = (keep - hi.astype(f32)).astype(bf16)
    sums = dot(hi, tri) + dot(lo, tri)
    w = jnp.where(allowed, jnp.exp(take + sums[:, 0:n]), 0.0).astype(bf16)
    return dot(w, vals), sums[:, n : 2 * n]


def tri_of(n):
    r = lax.broadcasted_iota(jnp.int32, (n, 2 * n), 0)
    c = lax.broadcasted_iota(jnp.int32, (n, 2 * n), 1)
    return jnp.where((r > c) | (c >= n), 1.0, 0.0).astype(bf16)


def finish(att, field, stats, c_gain, s_gain, out_w, mine, other, send, mix, n, per, members):
    ch = field.shape[1]
    mean = sum(st[0:1, :] for st in stats) / members
    m2 = sum(st[1:2, :] for st in stats)
    m2 = m2 + ch * sum((st[0:1, :] - mean) ** 2 for st in stats)
    rstd = lax.rsqrt(m2 / (ch * members) + norm_eps)
    mean_c = jnp.transpose(jnp.broadcast_to(mean, (ch, n)))
    rstd_c = jnp.transpose(jnp.broadcast_to(rstd, (ch, n)))
    z = (field[...] - mean_c) * rstd_c * c_gain[...]
    mix[:, 0:ch] = (z * jax.nn.sigmoid(z)).astype(bf16)
    ms = jnp.mean(att * att, axis=1, keepdims=True)
    normed = att * lax.rsqrt(ms + norm_eps)
    for h in range(per):
        part = normed[h * n : (h + 1) * n, :] * s_gain[h : h + 1, :]
        mix[:, ch + h * HEAD_DIM : ch + (h + 1) * HEAD_DIM] = part.astype(bf16)
    me = lax.axis_index("tp")
    rows = n // members
    lhs = jnp.concatenate(
        [mix[pl.ds(pl.multiple_of((me ^ k) * rows, rows), rows), :] for k in (0, 2, 1, 3)], axis=0
    )
    out = dot(lhs, out_w[...])
    mine[...] = out[0:rows, :]
    other[...] = out[rows : 2 * rows, :]
    send[...] = out[2 * rows :, :].astype(bf16)


def attend_kernel(*refs, blocks, members, n, per):
    q_ref = refs[0]
    pays = refs[1 : 1 + blocks]
    field = refs[1 + blocks]
    stats = refs[2 + blocks : 2 + blocks + members]
    c_gain, s_gain, out_w, mine, other, send, mix, parts, totals = refs[2 + blocks + members :]
    me = lax.axis_index("sp")
    q = q_ref[...]
    tri = tri_of(n)
    for k in range(blocks):
        j = me ^ k
        part, total = block_part(q, pays[k], (me - j) * n, n, per, tri)
        parts[pl.ds(j, 1)] = part[None]
        totals[pl.ds(j, 1)] = total[None]
    att = parts[blocks - 1]
    carry = totals[blocks - 1]
    for j in range(blocks - 2, -1, -1):
        att = att + jnp.exp(carry) * parts[j]
        if j:
            carry = carry + totals[j]
    finish(att, field, stats, c_gain, s_gain, out_w, mine, other, send, mix, n, per, members)


def attend_loop_kernel(*refs, members, n, per):
    q_ref, pays, field = refs[:3]
    stats = refs[3 : 3 + members]
    c_gain, s_gain, out_w, mine, other, send, mix = refs[3 + members :]
    me = lax.axis_index("sp")
    q = q_ref[...]
    tri = tri_of(n)

    def step(turn, carried):
        att, carry = carried
        j = me - turn
        part, total = block_part(q, pays.at[j], turn * n, n, per, tri)
        return att + jnp.exp(carry) * part, carry + total

    zero = jnp.zeros((per * n, HEAD_DIM), f32)
    att, _ = lax.fori_loop(0, me + 1, step, (zero, zero))
    finish(att, field, stats, c_gain, s_gain, out_w, mine, other, send, mix, n, per, members)


def call(body, outs, args, scratch=(), flops=0, spaces=None, limit=2**23):
    in_vmem = pl.BlockSpec(memory_space=pltpu.VMEM)
    if spaces is None:
        spaces = [True] * len(args)
    args = [
        pltpu.with_memory_space_constraint(arg, pltpu.VMEM) if held else arg
        for arg, held in zip(args, spaces)
    ]
    return pl.pallas_call(
        body,
        out_shape=[pltpu.VMEM(shape, dtype) for shape, dtype in outs],
        in_specs=[in_vmem] * len(args),
        out_specs=[in_vmem] * len(outs),
        scratch_shapes=scratch,
        cost_estimate=pl.CostEstimate(flops=flops, transcendentals=0, bytes_accessed=0),
        compiler_params=pltpu.CompilerParams(vmem_limit_bytes=limit),
    )(*args)


def shards(
    tokens,
    conv_input,
    conv_gate,
    query_weight,
    key_weight,
    value_weight,
    conv_taps,
    conv_gain,
    key_offsets,
    stick_gain,
    conv_output,
    stick_output,
):
    members = lax.axis_size("tp")
    blocks = lax.axis_size("sp")
    rows, width = tokens.shape
    n = rows * members
    ch = conv_input.shape[1]
    kv = key_weight.shape[1]
    query_cols = query_weight.shape[1]
    per = query_cols // kv
    off = jnp.pad(jnp.transpose(key_offsets), ((0, 16 - per), (0, 0)))
    by_core = swap(tokens, "tp", 1)
    by_chip = swap(tokens, "tp", 2)
    by_both = swap(by_chip, "tp", 1)
    in_vmem = pl.BlockSpec(memory_space=pltpu.VMEM)
    tok, conv_w, q_w, kv_w, taps, c_gain, off, s_gain, out_w = pl.pallas_call(
        load_kernel,
        out_shape=[
            pltpu.VMEM(shape, dtype)
            for shape, dtype in (
                ((rows, width), bf16),
                ((width, 2 * ch), bf16),
                ((width, query_cols), bf16),
                ((width, 2 * kv), bf16),
                (conv_taps.shape, f32),
                ((1, ch), f32),
                ((16, n), bf16),
                ((per, HEAD_DIM), f32),
                ((ch + query_cols, width), bf16),
            )
        ],
        in_specs=[pl.BlockSpec(memory_space=pltpu.HBM)] * 12,
        out_specs=[in_vmem] * 9,
        scratch_shapes=[pltpu.SemaphoreType.DMA((12,))],
        cost_estimate=pl.CostEstimate(flops=10**9, transcendentals=0, bytes_accessed=5 * 10**6),
        compiler_params=pltpu.CompilerParams(vmem_limit_bytes=2**21),
    )(
        tokens, conv_input, conv_gate, query_weight, key_weight, value_weight, conv_taps,
        conv_gain.reshape(1, ch), off, stick_gain.reshape(per, HEAD_DIM),
        conv_output, stick_output,
    )
    pay, qs, blend = call(
        project_kernel,
        [((n + 16, 2 * kv), bf16), ((per * n, HEAD_DIM), bf16), ((n, ch), bf16)],
        [tok, by_core, by_chip, by_both, conv_w, q_w, kv_w, off],
        scratch=[pltpu.VMEM((n, width), bf16)],
        flops=2 * n * width * (2 * ch + 4 * kv),
    )
    field_shapes = [((n, ch), f32), ((8, n), f32)]
    wide = [pltpu.VMEM((n + 32, ch), f32)]
    if blocks == 8:
        z6 = swap(pay, "sp", 6)
        z2 = swap(pay, "sp", 2)
        z4 = swap(pay, "sp", 4)
        x1 = swap(pay, "sp", 1)
        x7 = swap(z6, "sp", 1)
        x3 = swap(z2, "sp", 1)
        x5 = swap(z4, "sp", 1)
        pays = [pay, x1, z2, x3, z4, x5, z6, x7]
        conv_args = [x1, x3, x7, blend, taps]
        field, stats = call(conv_kernel, field_shapes, conv_args, wide, 64 * n * ch)
    else:
        pays = [lax.all_gather(pay, "sp", axis=0)]
        halo = from_behind(blend[n - 32 :], "sp", 1)
        conv_args = [halo, blend, taps]
        field, stats = call(conv_plain_kernel, field_shapes, conv_args, wide, 64 * n * ch)
    stats_chip = swap(stats, "tp", 2)
    all_stats = [stats, swap(stats, "tp", 1), stats_chip, swap(stats_chip, "tp", 1)]
    scratch = [pltpu.VMEM((n, ch + query_cols), bf16)]
    if blocks == 8:
        body = functools.partial(attend_kernel, blocks=blocks, members=members, n=n, per=per)
        scratch += [pltpu.VMEM((blocks, per * n, HEAD_DIM), f32)] * 2
    else:
        body = functools.partial(attend_loop_kernel, members=members, n=n, per=per)
    args = [qs, *pays, field, *all_stats, c_gain, s_gain, out_w]
    mine, other, send = call(
        body,
        [((rows, width), f32), ((rows, width), f32), ((2 * rows, width), bf16)],
        args,
        scratch=scratch,
        flops=2 * n * width * (ch + query_cols),
        limit=2**23 if blocks == 8 else 2**25,
        spaces=[True] + [blocks == 8] * len(pays) + [True] * (len(args) - 1 - len(pays)),
    )
    got = swap(send, "tp", 1).astype(f32)
    chip = swap((other + got[rows:]).astype(bf16), "tp", 2)
    return (mine + got[:rows] + chip.astype(f32)).astype(bf16)


def solution(mesh):
    return jax.shard_map(
        shards,
        mesh=mesh,
        in_specs=(
            P(("sp", "tp"), None),
            P(None, "tp"),
            P(None, "tp"),
            P(None, "tp"),
            P(None, "tp"),
            P(None, "tp"),
            P(None, "tp"),
            P("tp"),
            P("sp", "tp"),
            P("tp"),
            P("tp", None),
            P("tp", None),
        ),
        out_specs=P(("sp", "tp"), None),
        check_vma=False,
    )
```

```python
import functools

import jax
import jax.numpy as jnp
from jax import lax
from jax.experimental import pallas as pl
from jax.experimental.pallas import tpu as pltpu
from jax.sharding import PartitionSpec as P

HEAD_DIM = 128
norm_eps = 1e-05
f32 = jnp.float32
bf16 = jnp.bfloat16


def swap(value, axis, by):
    count = lax.axis_size(axis)
    return lax.ppermute(value, axis, [(i, i ^ by) for i in range(count)])


def from_behind(value, axis, by):
    count = lax.axis_size(axis)
    pairs = [(i, i + by) for i in range(count) if 0 <= i + by < count]
    return lax.ppermute(value, axis, pairs)


def dot(a, b):
    return jnp.dot(a, b, preferred_element_type=f32)


def load_kernel(*refs):
    sources, sems = refs[:12], refs[-1]
    tokens, w_in, w_gate, w_q, w_k, w_v, taps, c_gain, off, s_gain, w_c, w_s = sources
    tok, conv_w, q_w, kv_w, taps_v, c_gain_v, off_v, s_gain_v, out_w = refs[12:-1]
    ch = w_in.shape[1]
    kv = w_k.shape[1]
    pairs = [
        (w_k, kv_w.at[:, 0:kv]),
        (w_v, kv_w.at[:, kv:]),
        (w_q, q_w),
        (w_in, conv_w.at[:, 0:ch]),
        (w_gate, conv_w.at[:, ch:]),
        (tokens, tok),
        (taps, taps_v),
        (c_gain, c_gain_v),
        (off, off_v),
        (s_gain, s_gain_v),
        (w_c, out_w.at[0:ch]),
        (w_s, out_w.at[ch:]),
    ]
    copies = [pltpu.make_async_copy(a, b, sems.at[i]) for i, (a, b) in enumerate(pairs)]
    for copy in copies:
        copy.start()
    for copy in copies:
        copy.wait()


def project_kernel(t0, t1, t2, t3, conv_w, q_w, kv_w, off, pay, qs, blend, x_all):
    rows = t0.shape[0]
    me = lax.axis_index("tp")
    for k, t in enumerate((t0, t1, t2, t3)):
        x_all[pl.ds(pl.multiple_of((me ^ k) * rows, rows), rows), :] = t[...]
    x = x_all[...]
    n = x.shape[0]
    ch = conv_w.shape[1] // 2
    kv = kv_w.shape[1] // 2
    pay[0:n, :] = dot(x, kv_w[...]).astype(bf16)
    q = dot(x, q_w[...]).astype(bf16)
    for h in range(q.shape[1] // HEAD_DIM):
        qs[h * n : (h + 1) * n, :] = q[:, h * HEAD_DIM : (h + 1) * HEAD_DIM]
    both = dot(x, conv_w[...]).astype(bf16).astype(f32)
    b = (both[:, 0:ch] * jax.nn.sigmoid(both[:, ch:])).astype(bf16)
    blend[...] = b
    row = lax.broadcasted_iota(jnp.int32, (16, kv), 0)
    pay[n:, 0:kv] = jnp.where(row < 2, off[...], b[n - 32 : n - 16, :])
    pay[n:, kv:] = b[n - 16 :, :]


def conv_kernel(p1, p3, p7, blend, taps, field, stats, wide):
    n = blend.shape[0]
    half = p1.shape[1] // 2
    reach = taps.shape[0] - 1
    me = lax.axis_index("sp")
    flip = me ^ (me - 1)
    halo = jnp.where(flip == 1, p1[n:, :], jnp.where(flip == 3, p3[n:, :], p7[n:, :]))
    halo = jnp.where(me > 0, halo.astype(f32), 0.0)
    wide[0:16, :] = halo[:, 0:half]
    wide[16:32, :] = halo[:, half:]
    convolve(blend, taps, field, stats, wide)


def conv_plain_kernel(halo, blend, taps, field, stats, wide):
    wide[0:32, :] = halo[...].astype(f32)
    convolve(blend, taps, field, stats, wide)


def convolve(blend, taps, field, stats, wide):
    n = blend.shape[0]
    reach = taps.shape[0] - 1
    wide[32 : 32 + n, :] = blend[...].astype(f32)
    base = 32 - reach
    f = taps[0:1, :] * wide[base : base + n, :]
    for t in range(1, reach + 1):
        f = f + taps[t : t + 1, :] * wide[base + t : base + t + n, :]
    field[...] = f
    ch = f.shape[1]
    mean = jnp.sum(f, axis=1, keepdims=True) / ch
    d = f - mean
    m2 = jnp.sum(d * d, axis=1, keepdims=True)
    stats[0:1, :] = jnp.transpose(jnp.broadcast_to(mean, (n, 128)))[0:1, :]
    stats[1:2, :] = jnp.transpose(jnp.broadcast_to(m2, (n, 128)))[0:1, :]


def block_part(q, pay, gap, n, per, tri):
    kv = HEAD_DIM
    keys = pay[0:n, 0:kv]
    vals = pay[0:n, kv : 2 * kv]
    off = pay[n : n + 16, 0:kv].astype(f32)
    s = lax.dot_general(q, keys, (((1,), (1,)), ((), ())), preferred_element_type=f32)
    s = s * (HEAD_DIM ** (-0.5))
    shift = jnp.concatenate(
        [jnp.broadcast_to(off[h : h + 1, :], (n, n)) for h in range(per)], axis=0
    )
    s = s + shift
    row = lax.broadcasted_iota(jnp.int32, s.shape, 0) & (n - 1)
    col = lax.broadcasted_iota(jnp.int32, s.shape, 1)
    allowed = col < row + gap
    soft = jnp.log1p(jnp.exp(-jnp.abs(s)))
    take = jnp.minimum(s, 0.0) - soft
    keep = jnp.where(allowed, jnp.minimum(-s, 0.0) - soft, 0.0)
    hi = keep.astype(bf16)
    lo = (keep - hi.astype(f32)).astype(bf16)
    sums = dot(hi, tri) + dot(lo, tri)
    w = jnp.where(allowed, jnp.exp(take + sums[:, 0:n]), 0.0).astype(bf16)
    return dot(w, vals), sums[:, n : 2 * n]


def tri_of(n):
    r = lax.broadcasted_iota(jnp.int32, (n, 2 * n), 0)
    c = lax.broadcasted_iota(jnp.int32, (n, 2 * n), 1)
    return jnp.where((r > c) | (c >= n), 1.0, 0.0).astype(bf16)


def finish(att, field, stats, c_gain, s_gain, out_w, mine, other, send, mix, n, per, members):
    ch = field.shape[1]
    mean = sum(st[0:1, :] for st in stats) / members
    m2 = sum(st[1:2, :] for st in stats)
    m2 = m2 + ch * sum((st[0:1, :] - mean) ** 2 for st in stats)
    rstd = lax.rsqrt(m2 / (ch * members) + norm_eps)
    mean_c = jnp.transpose(jnp.broadcast_to(mean, (ch, n)))
    rstd_c = jnp.transpose(jnp.broadcast_to(rstd, (ch, n)))
    z = (field[...] - mean_c) * rstd_c * c_gain[...]
    mix[:, 0:ch] = (z * jax.nn.sigmoid(z)).astype(bf16)
    ms = jnp.mean(att * att, axis=1, keepdims=True)
    normed = att * lax.rsqrt(ms + norm_eps)
    for h in range(per):
        part = normed[h * n : (h + 1) * n, :] * s_gain[h : h + 1, :]
        mix[:, ch + h * HEAD_DIM : ch + (h + 1) * HEAD_DIM] = part.astype(bf16)
    me = lax.axis_index("tp")
    rows = n // members
    lhs = jnp.concatenate(
        [mix[pl.ds(pl.multiple_of((me ^ k) * rows, rows), rows), :] for k in (0, 2, 1, 3)], axis=0
    )
    out = dot(lhs, out_w[...])
    mine[...] = out[0:rows, :]
    other[...] = out[rows : 2 * rows, :]
    send[...] = out[2 * rows :, :].astype(bf16)


def attend_kernel(*refs, blocks, members, n, per):
    q_ref = refs[0]
    pays = refs[1 : 1 + blocks]
    field = refs[1 + blocks]
    stats = refs[2 + blocks : 2 + blocks + members]
    c_gain, s_gain, out_w, mine, other, send, mix, parts, totals = refs[2 + blocks + members :]
    me = lax.axis_index("sp")
    q = q_ref[...]
    tri = tri_of(n)
    for k in range(blocks):
        j = me ^ k
        part, total = block_part(q, pays[k], (me - j) * n, n, per, tri)
        parts[pl.ds(j, 1)] = part[None]
        totals[pl.ds(j, 1)] = total[None]
    att = parts[blocks - 1]
    carry = totals[blocks - 1]
    for j in range(blocks - 2, -1, -1):
        att = att + jnp.exp(carry) * parts[j]
        if j:
            carry = carry + totals[j]
    finish(att, field, stats, c_gain, s_gain, out_w, mine, other, send, mix, n, per, members)


def attend_loop_kernel(*refs, members, n, per):
    q_ref, pays, field = refs[:3]
    stats = refs[3 : 3 + members]
    c_gain, s_gain, out_w, mine, other, send, mix = refs[3 + members :]
    me = lax.axis_index("sp")
    q = q_ref[...]
    tri = tri_of(n)

    def step(turn, carried):
        att, carry = carried
        j = me - turn
        part, total = block_part(q, pays.at[j], turn * n, n, per, tri)
        return att + jnp.exp(carry) * part, carry + total

    zero = jnp.zeros((per * n, HEAD_DIM), f32)
    att, _ = lax.fori_loop(0, me + 1, step, (zero, zero))
    finish(att, field, stats, c_gain, s_gain, out_w, mine, other, send, mix, n, per, members)


def call(body, outs, args, scratch=(), flops=0, spaces=None, limit=2**23):
    in_vmem = pl.BlockSpec(memory_space=pltpu.VMEM)
    if spaces is None:
        spaces = [True] * len(args)
    args = [
        pltpu.with_memory_space_constraint(arg, pltpu.VMEM) if held else arg
        for arg, held in zip(args, spaces)
    ]
    return pl.pallas_call(
        body,
        out_shape=[pltpu.VMEM(shape, dtype) for shape, dtype in outs],
        in_specs=[in_vmem] * len(args),
        out_specs=[in_vmem] * len(outs),
        scratch_shapes=scratch,
        cost_estimate=pl.CostEstimate(flops=flops, transcendentals=0, bytes_accessed=0),
        compiler_params=pltpu.CompilerParams(vmem_limit_bytes=limit),
    )(*args)


def shards(
    tokens,
    conv_input,
    conv_gate,
    query_weight,
    key_weight,
    value_weight,
    conv_taps,
    conv_gain,
    key_offsets,
    stick_gain,
    conv_output,
    stick_output,
):
    members = lax.axis_size("tp")
    blocks = lax.axis_size("sp")
    rows, width = tokens.shape
    n = rows * members
    ch = conv_input.shape[1]
    kv = key_weight.shape[1]
    query_cols = query_weight.shape[1]
    per = query_cols // kv
    off = jnp.pad(jnp.transpose(key_offsets), ((0, 16 - per), (0, 0)))
    by_core = swap(tokens, "tp", 1)
    by_chip = swap(tokens, "tp", 2)
    in_vmem = pl.BlockSpec(memory_space=pltpu.VMEM)
    sources = [
        tokens, conv_input, conv_gate, query_weight, key_weight, value_weight, conv_taps,
        conv_gain.reshape(1, ch), off, stick_gain.reshape(per, HEAD_DIM),
        conv_output, stick_output,
    ]
    tok, conv_w, q_w, kv_w, taps, c_gain, off, s_gain, out_w = pl.pallas_call(
        load_kernel,
        out_shape=[
            pltpu.VMEM(shape, dtype)
            for shape, dtype in (
                ((rows, width), bf16),
                ((width, 2 * ch), bf16),
                ((width, query_cols), bf16),
                ((width, 2 * kv), bf16),
                (conv_taps.shape, f32),
                ((1, ch), f32),
                ((16, n), bf16),
                ((per, HEAD_DIM), f32),
                ((ch + query_cols, width), bf16),
            )
        ],
        in_specs=[pl.BlockSpec(memory_space=pltpu.HBM)] * 12,
        out_specs=[in_vmem] * 9,
        scratch_shapes=[pltpu.SemaphoreType.DMA((12,))],
        cost_estimate=pl.CostEstimate(flops=10**9, transcendentals=0, bytes_accessed=5 * 10**6),
        compiler_params=pltpu.CompilerParams(vmem_limit_bytes=2**21),
    )(*[pltpu.with_memory_space_constraint(source, pltpu.HBM) for source in sources])
    by_chip, tok = lax.optimization_barrier((by_chip, tok))
    by_both = swap(by_chip, "tp", 1)
    pay, qs, blend = call(
        project_kernel,
        [((n + 16, 2 * kv), bf16), ((per * n, HEAD_DIM), bf16), ((n, ch), bf16)],
        [tok, by_core, by_chip, by_both, conv_w, q_w, kv_w, off],
        scratch=[pltpu.VMEM((n, width), bf16)],
        flops=2 * n * width * (2 * ch + 4 * kv),
    )
    field_shapes = [((n, ch), f32), ((8, n), f32)]
    wide = [pltpu.VMEM((n + 32, ch), f32)]
    if blocks == 8:
        z2 = swap(pay, "sp", 2)
        z6 = swap(pay, "sp", 6)
        z4 = swap(pay, "sp", 4)
        x1 = swap(pay, "sp", 1)
        x3 = swap(z2, "sp", 1)
        x7 = swap(z6, "sp", 1)
        x5 = swap(z4, "sp", 1)
        pays = [pay, x1, z2, x3, z4, x5, z6, x7]
        conv_args = [x1, x3, x7, blend, taps]
        field, stats = call(conv_kernel, field_shapes, conv_args, wide, 64 * n * ch)
    else:
        pays = [lax.all_gather(pay, "sp", axis=0)]
        halo = from_behind(blend[n - 32 :], "sp", 1)
        conv_args = [halo, blend, taps]
        field, stats = call(conv_plain_kernel, field_shapes, conv_args, wide, 64 * n * ch)
    stats_chip = swap(stats, "tp", 2)
    all_stats = [stats, swap(stats, "tp", 1), stats_chip, swap(stats_chip, "tp", 1)]
    scratch = [pltpu.VMEM((n, ch + query_cols), bf16)]
    if blocks == 8:
        body = functools.partial(attend_kernel, blocks=blocks, members=members, n=n, per=per)
        scratch += [pltpu.VMEM((blocks, per * n, HEAD_DIM), f32)] * 2
    else:
        body = functools.partial(attend_loop_kernel, members=members, n=n, per=per)
    args = [qs, *pays, field, *all_stats, c_gain, s_gain, out_w]
    mine, other, send = call(
        body,
        [((rows, width), f32), ((rows, width), f32), ((2 * rows, width), bf16)],
        args,
        scratch=scratch,
        flops=2 * n * width * (ch + query_cols),
        limit=2**23 if blocks == 8 else 2**25,
        spaces=[True] + [blocks == 8] * len(pays) + [True] * (len(args) - 1 - len(pays)),
    )
    got = swap(send, "tp", 1).astype(f32)
    chip = swap((other + got[rows:]).astype(bf16), "tp", 2)
    return (mine + got[:rows] + chip.astype(f32)).astype(bf16)


def solution(mesh):
    return jax.shard_map(
        shards,
        mesh=mesh,
        in_specs=(
            P(("sp", "tp"), None),
            P(None, "tp"),
            P(None, "tp"),
            P(None, "tp"),
            P(None, "tp"),
            P(None, "tp"),
            P(None, "tp"),
            P("tp"),
            P("sp", "tp"),
            P("tp"),
            P("tp", None),
            P("tp", None),
        ),
        out_specs=P(("sp", "tp"), None),
        check_vma=False,
    )
```

```python
import functools

import jax
import jax.numpy as jnp
from jax import lax
from jax.experimental import pallas as pl
from jax.experimental.pallas import tpu as pltpu
from jax.sharding import PartitionSpec as P

HEAD_DIM = 128
norm_eps = 1e-05
f32 = jnp.float32
bf16 = jnp.bfloat16


def swap(value, axis, by):
    count = lax.axis_size(axis)
    return lax.ppermute(value, axis, [(i, i ^ by) for i in range(count)])


def from_behind(value, axis, by):
    count = lax.axis_size(axis)
    pairs = [(i, i + by) for i in range(count) if 0 <= i + by < count]
    return lax.ppermute(value, axis, pairs)


def dot(a, b):
    return jnp.dot(a, b, preferred_element_type=f32)


def load_kernel(*refs):
    sources, sems = refs[:12], refs[-1]
    tokens, w_in, w_gate, w_q, w_k, w_v, taps, c_gain, off, s_gain, w_c, w_s = sources
    tok, conv_w, q_w, kv_w, taps_v, c_gain_v, off_v, s_gain_v, out_w = refs[12:-1]
    ch = w_in.shape[1]
    kv = w_k.shape[1]
    pairs = [
        (w_k, kv_w.at[:, 0:kv]),
        (w_v, kv_w.at[:, kv:]),
        (w_q, q_w),
        (w_in, conv_w.at[:, 0:ch]),
        (w_gate, conv_w.at[:, ch:]),
        (tokens, tok),
        (taps, taps_v),
        (c_gain, c_gain_v),
        (off, off_v),
        (s_gain, s_gain_v),
        (w_c, out_w.at[0:ch]),
        (w_s, out_w.at[ch:]),
    ]
    copies = [pltpu.make_async_copy(a, b, sems.at[i]) for i, (a, b) in enumerate(pairs)]
    for copy in copies:
        copy.start()
    for copy in copies:
        copy.wait()


def project_kernel(t0, t1, t2, t3, conv_w, q_w, kv_w, off, pay, qs, blend, x_all):
    rows = t0.shape[0]
    me = lax.axis_index("tp")
    for k, t in enumerate((t0, t1, t2, t3)):
        x_all[pl.ds(pl.multiple_of((me ^ k) * rows, rows), rows), :] = t[...]
    x = x_all[...]
    n = x.shape[0]
    ch = conv_w.shape[1] // 2
    kv = kv_w.shape[1] // 2
    pay[0:n, :] = dot(x, kv_w[...]).astype(bf16)
    q = dot(x, q_w[...]).astype(bf16)
    for h in range(q.shape[1] // HEAD_DIM):
        qs[h * n : (h + 1) * n, :] = q[:, h * HEAD_DIM : (h + 1) * HEAD_DIM]
    both = dot(x, conv_w[...]).astype(bf16).astype(f32)
    b = (both[:, 0:ch] * jax.nn.sigmoid(both[:, ch:])).astype(bf16)
    blend[...] = b
    row = lax.broadcasted_iota(jnp.int32, (16, kv), 0)
    pay[n:, 0:kv] = jnp.where(row < 2, off[...], b[n - 32 : n - 16, :])
    pay[n:, kv:] = b[n - 16 :, :]


def conv_kernel(p1, p3, p7, blend, taps, field, stats, wide):
    n = blend.shape[0]
    half = p1.shape[1] // 2
    reach = taps.shape[0] - 1
    me = lax.axis_index("sp")
    flip = me ^ (me - 1)
    halo = jnp.where(flip == 1, p1[n:, :], jnp.where(flip == 3, p3[n:, :], p7[n:, :]))
    halo = jnp.where(me > 0, halo.astype(f32), 0.0)
    wide[0:16, :] = halo[:, 0:half]
    wide[16:32, :] = halo[:, half:]
    convolve(blend, taps, field, stats, wide)


def conv_plain_kernel(halo, blend, taps, field, stats, wide):
    wide[0:32, :] = halo[...].astype(f32)
    convolve(blend, taps, field, stats, wide)


def convolve(blend, taps, field, stats, wide):
    n = blend.shape[0]
    reach = taps.shape[0] - 1
    wide[32 : 32 + n, :] = blend[...].astype(f32)
    base = 32 - reach
    f = taps[0:1, :] * wide[base : base + n, :]
    for t in range(1, reach + 1):
        f = f + taps[t : t + 1, :] * wide[base + t : base + t + n, :]
    field[...] = f
    ch = f.shape[1]
    mean = jnp.sum(f, axis=1, keepdims=True) / ch
    d = f - mean
    m2 = jnp.sum(d * d, axis=1, keepdims=True)
    stats[0:1, :] = jnp.transpose(jnp.broadcast_to(mean, (n, 128)))[0:1, :]
    stats[1:2, :] = jnp.transpose(jnp.broadcast_to(m2, (n, 128)))[0:1, :]


def block_part(q, pay, gap, n, per, tri):
    kv = HEAD_DIM
    keys = pay[0:n, 0:kv]
    vals = pay[0:n, kv : 2 * kv]
    off = pay[n : n + 16, 0:kv].astype(f32)
    s = lax.dot_general(q, keys, (((1,), (1,)), ((), ())), preferred_element_type=f32)
    s = s * (HEAD_DIM ** (-0.5))
    shift = jnp.concatenate(
        [jnp.broadcast_to(off[h : h + 1, :], (n, n)) for h in range(per)], axis=0
    )
    s = s + shift
    row = lax.broadcasted_iota(jnp.int32, s.shape, 0) & (n - 1)
    col = lax.broadcasted_iota(jnp.int32, s.shape, 1)
    allowed = col < row + gap
    soft = jnp.log1p(jnp.exp(-jnp.abs(s)))
    take = jnp.minimum(s, 0.0) - soft
    keep = jnp.where(allowed, jnp.minimum(-s, 0.0) - soft, 0.0)
    hi = keep.astype(bf16)
    lo = (keep - hi.astype(f32)).astype(bf16)
    sums = dot(hi, tri) + dot(lo, tri)
    w = jnp.where(allowed, jnp.exp(take + sums[:, 0:n]), 0.0).astype(bf16)
    return dot(w, vals), sums[:, n : 2 * n]


def tri_of(n):
    r = lax.broadcasted_iota(jnp.int32, (n, 2 * n), 0)
    c = lax.broadcasted_iota(jnp.int32, (n, 2 * n), 1)
    return jnp.where((r > c) | (c >= n), 1.0, 0.0).astype(bf16)


def normed_heads(att, s_gain, mix, n, per):
    ms = jnp.mean(att * att, axis=1, keepdims=True)
    normed = att * lax.rsqrt(ms + norm_eps)
    for h in range(per):
        part = normed[h * n : (h + 1) * n, :] * s_gain[h : h + 1, :]
        mix[:, h * HEAD_DIM : (h + 1) * HEAD_DIM] = part.astype(bf16)


def by_slot(mix, n, members):
    me = lax.axis_index("tp")
    rows = n // members
    picks = [mix[pl.ds(pl.multiple_of((me ^ k) * rows, rows), rows), :] for k in (0, 2, 1, 3)]
    return jnp.concatenate(picks, axis=0)


def parts_kernel(*refs, slots, blocks, n, per):
    q_ref = refs[0]
    pays = refs[1 : 1 + len(slots)]
    sums = refs[-1]
    me = lax.axis_index("sp")
    q = q_ref[...]
    tri = tri_of(n)
    for k, pay in zip(slots, pays):
        j = me ^ k
        part, total = block_part(q, pay, (me - j) * n, n, per, tri)
        sums[pl.ds(j, 1)] = part[None]
        sums[pl.ds(blocks + j, 1)] = total[None]


def stick_kernel(q_ref, pay, sums_in, s_gain, out_w, stick, mix, *, slot, blocks, members, n, per):
    me = lax.axis_index("sp")
    last = me ^ slot
    part, total = block_part(q_ref[...], pay, (me - last) * n, n, per, tri_of(n))
    att = jnp.zeros_like(part)
    carry = jnp.zeros_like(total)
    for j in range(blocks - 1, -1, -1):
        here = last == j
        att = att + jnp.exp(carry) * jnp.where(here, part, sums_in[j])
        if j:
            carry = carry + jnp.where(here, total, sums_in[blocks + j])
    normed_heads(att, s_gain, mix, n, per)
    ch = out_w.shape[0] - per * HEAD_DIM
    stick[...] = dot(by_slot(mix, n, members), out_w[ch:, :])


def stick_loop_kernel(q_ref, pays, s_gain, out_w, stick, mix, *, members, n, per):
    me = lax.axis_index("sp")
    q = q_ref[...]
    tri = tri_of(n)

    def step(turn, carried):
        att, carry = carried
        part, total = block_part(q, pays.at[me - turn], turn * n, n, per, tri)
        return att + jnp.exp(carry) * part, carry + total

    zero = jnp.zeros((per * n, HEAD_DIM), f32)
    att, _ = lax.fori_loop(0, me + 1, step, (zero, zero))
    normed_heads(att, s_gain, mix, n, per)
    ch = out_w.shape[0] - per * HEAD_DIM
    stick[...] = dot(by_slot(mix, n, members), out_w[ch:, :])


def finish_kernel(field, s0, s1, s2, s3, c_gain, out_w, stick, mine, other, send, mix, *, members):
    n, ch = field.shape
    stats = (s0, s1, s2, s3)
    mean = sum(st[0:1, :] for st in stats) / members
    m2 = sum(st[1:2, :] for st in stats)
    m2 = m2 + ch * sum((st[0:1, :] - mean) ** 2 for st in stats)
    rstd = lax.rsqrt(m2 / (ch * members) + norm_eps)
    mean_c = jnp.transpose(jnp.broadcast_to(mean, (ch, n)))
    rstd_c = jnp.transpose(jnp.broadcast_to(rstd, (ch, n)))
    z = (field[...] - mean_c) * rstd_c * c_gain[...]
    mix[...] = (z * jax.nn.sigmoid(z)).astype(bf16)
    out = dot(by_slot(mix, n, members), out_w[0:ch, :]) + stick[...]
    rows = n // members
    mine[...] = out[0:rows, :]
    other[...] = out[rows : 2 * rows, :]
    send[...] = out[2 * rows :, :].astype(bf16)


def call(body, outs, args, scratch=(), flops=0, spaces=None, limit=2**22, aliases={}):
    in_vmem = pl.BlockSpec(memory_space=pltpu.VMEM)
    if spaces is None:
        spaces = [True] * len(args)
    args = [
        pltpu.with_memory_space_constraint(arg, pltpu.VMEM) if held else arg
        for arg, held in zip(args, spaces)
    ]
    return pl.pallas_call(
        body,
        out_shape=[pltpu.VMEM(shape, dtype) for shape, dtype in outs],
        in_specs=[in_vmem] * len(args),
        out_specs=[in_vmem] * len(outs),
        scratch_shapes=scratch,
        input_output_aliases=aliases,
        name=getattr(body, "func", body).__name__,
        cost_estimate=pl.CostEstimate(flops=flops, transcendentals=0, bytes_accessed=0),
        compiler_params=pltpu.CompilerParams(vmem_limit_bytes=limit),
    )(*args)


def shards(
    tokens,
    conv_input,
    conv_gate,
    query_weight,
    key_weight,
    value_weight,
    conv_taps,
    conv_gain,
    key_offsets,
    stick_gain,
    conv_output,
    stick_output,
):
    members = lax.axis_size("tp")
    blocks = lax.axis_size("sp")
    rows, width = tokens.shape
    n = rows * members
    ch = conv_input.shape[1]
    kv = key_weight.shape[1]
    query_cols = query_weight.shape[1]
    per = query_cols // kv
    off = jnp.pad(jnp.transpose(key_offsets), ((0, 16 - per), (0, 0)))
    by_core = swap(tokens, "tp", 1)
    by_chip = swap(tokens, "tp", 2)
    in_vmem = pl.BlockSpec(memory_space=pltpu.VMEM)
    sources = [
        tokens, conv_input, conv_gate, query_weight, key_weight, value_weight, conv_taps,
        conv_gain.reshape(1, ch), off, stick_gain.reshape(per, HEAD_DIM),
        conv_output, stick_output,
    ]
    tok, conv_w, q_w, kv_w, taps, c_gain, off, s_gain, out_w = pl.pallas_call(
        load_kernel,
        out_shape=[
            pltpu.VMEM(shape, dtype)
            for shape, dtype in (
                ((rows, width), bf16),
                ((width, 2 * ch), bf16),
                ((width, query_cols), bf16),
                ((width, 2 * kv), bf16),
                (conv_taps.shape, f32),
                ((1, ch), f32),
                ((16, n), bf16),
                ((per, HEAD_DIM), f32),
                ((ch + query_cols, width), bf16),
            )
        ],
        in_specs=[pl.BlockSpec(memory_space=pltpu.HBM)] * 12,
        out_specs=[in_vmem] * 9,
        scratch_shapes=[pltpu.SemaphoreType.DMA((12,))],
        cost_estimate=pl.CostEstimate(flops=10**9, transcendentals=0, bytes_accessed=5 * 10**6),
        compiler_params=pltpu.CompilerParams(vmem_limit_bytes=2**21),
    )(*[pltpu.with_memory_space_constraint(source, pltpu.HBM) for source in sources])
    by_chip, tok = lax.optimization_barrier((by_chip, tok))
    by_both = swap(by_chip, "tp", 1)
    pay, qs, blend = call(
        project_kernel,
        [((n + 16, 2 * kv), bf16), ((per * n, HEAD_DIM), bf16), ((n, ch), bf16)],
        [tok, by_core, by_chip, by_both, conv_w, q_w, kv_w, off],
        scratch=[pltpu.VMEM((n, width), bf16)],
        flops=2 * n * width * (2 * ch + 4 * kv),
    )
    field_shapes = [((n, ch), f32), ((8, n), f32)]
    wide = [pltpu.VMEM((n + 32, ch), f32)]
    sizes = dict(n=n, per=per)
    heads = per * n
    mixed = [pltpu.VMEM((n, query_cols), bf16)]
    block_flops = 2 * heads * n * HEAD_DIM * 8
    if blocks == 8:
        z2 = swap(pay, "sp", 2)
        z6 = swap(pay, "sp", 6)
        z4 = swap(pay, "sp", 4)
        x1 = swap(pay, "sp", 1)
        x7 = swap(z6, "sp", 1)
        x3 = swap(z2, "sp", 1)
        x5 = swap(z4, "sp", 1)

        def parts(slots, pays, sums):
            args = [qs, *pays] + ([] if sums is None else [sums])
            (out,) = call(
                functools.partial(parts_kernel, slots=slots, blocks=blocks, **sizes),
                [((2 * blocks, heads, HEAD_DIM), f32)],
                args,
                flops=len(slots) * block_flops,
                aliases={} if sums is None else {len(args) - 1: 0},
            )
            return out

        sums = parts((0,), (pay,), None)
        sums = parts((2, 6, 1), (z2, z6, x1), sums)
        sums = parts((4,), (z4,), sums)
        conv_args = [x1, x3, x7, blend, taps]
        field, stats = call(conv_kernel, field_shapes, conv_args, wide, 64 * n * ch)
        all_stats = [stats] + [swap(stats, "tp", k) for k in (2, 3, 1)]
        sums = parts((7, 3), (x7, x3), sums)
        body = functools.partial(stick_kernel, slot=5, blocks=blocks, members=members, **sizes)
        stick_args = [qs, x5, sums, s_gain, out_w]
        spaces = None
    else:
        pays = lax.all_gather(pay, "sp", axis=0)
        halo = from_behind(blend[n - 32 :], "sp", 1)
        field, stats = call(
            conv_plain_kernel, field_shapes, [halo, blend, taps], wide, 64 * n * ch
        )
        all_stats = [stats] + [swap(stats, "tp", k) for k in (2, 3, 1)]
        body = functools.partial(stick_loop_kernel, members=members, **sizes)
        stick_args = [qs, pays, s_gain, out_w]
        spaces = [True, False, True, True]
    (stick,) = call(
        body,
        [((n, width), f32)],
        stick_args,
        scratch=mixed,
        flops=block_flops + 2 * n * width * query_cols,
        spaces=spaces,
        limit=2**22 if blocks == 8 else 2**25,
    )
    mine, other, send = call(
        functools.partial(finish_kernel, members=members),
        [((rows, width), f32), ((rows, width), f32), ((2 * rows, width), bf16)],
        [field, *all_stats, c_gain, out_w, stick],
        scratch=[pltpu.VMEM((n, ch), bf16)],
        flops=2 * n * width * ch,
    )
    got = swap(send, "tp", 1).astype(f32)
    chip = swap((other + got[rows:]).astype(bf16), "tp", 2)
    return (mine + got[:rows] + chip.astype(f32)).astype(bf16)


def solution(mesh):
    return jax.shard_map(
        shards,
        mesh=mesh,
        in_specs=(
            P(("sp", "tp"), None),
            P(None, "tp"),
            P(None, "tp"),
            P(None, "tp"),
            P(None, "tp"),
            P(None, "tp"),
            P(None, "tp"),
            P("tp"),
            P("sp", "tp"),
            P("tp"),
            P("tp", None),
            P("tp", None),
        ),
        out_specs=P(("sp", "tp"), None),
        check_vma=False,
    )
```

```python
import functools

import jax
import jax.numpy as jnp
from jax import lax
from jax.experimental import pallas as pl
from jax.experimental.pallas import tpu as pltpu
from jax.sharding import PartitionSpec as P

HEAD_DIM = 128
LOG2E = 1.4426950408889634
norm_eps = 1e-05
f32 = jnp.float32
bf16 = jnp.bfloat16


def swap(value, axis, by):
    count = lax.axis_size(axis)
    return lax.ppermute(value, axis, [(i, i ^ by) for i in range(count)])


def from_behind(value, axis, by):
    count = lax.axis_size(axis)
    pairs = [(i, i + by) for i in range(count) if 0 <= i + by < count]
    return lax.ppermute(value, axis, pairs)


def dot(a, b):
    return jnp.dot(a, b, preferred_element_type=f32)


def load_kernel(*refs):
    sources, sems = refs[:12], refs[-1]
    tokens, w_in, w_gate, w_q, w_k, w_v, taps, c_gain, off, s_gain, w_c, w_s = sources
    tok, conv_w, q_w, kv_w, taps_v, c_gain_v, off_v, s_gain_v, out_w = refs[12:-1]
    ch = w_in.shape[1]
    kv = w_k.shape[1]
    pairs = [
        (w_k, kv_w.at[:, 0:kv]),
        (w_v, kv_w.at[:, kv:]),
        (w_q, q_w),
        (w_in, conv_w.at[:, 0:ch]),
        (w_gate, conv_w.at[:, ch:]),
        (tokens, tok),
        (taps, taps_v),
        (c_gain, c_gain_v),
        (off, off_v),
        (s_gain, s_gain_v),
        (w_c, out_w.at[0:ch]),
        (w_s, out_w.at[ch:]),
    ]
    copies = [pltpu.make_async_copy(a, b, sems.at[i]) for i, (a, b) in enumerate(pairs)]
    for copy in copies:
        copy.start()
    for copy in copies:
        copy.wait()


def project_kernel(t0, t1, t2, t3, conv_w, q_w, kv_w, off, pay, qs, blend, x_all):
    rows = t0.shape[0]
    me = lax.axis_index("tp")
    for k, t in enumerate((t0, t1, t2, t3)):
        x_all[pl.ds(pl.multiple_of((me ^ k) * rows, rows), rows), :] = t[...]
    x = x_all[...]
    n = x.shape[0]
    ch = conv_w.shape[1] // 2
    kv = kv_w.shape[1] // 2
    pay[0:n, :] = dot(x, kv_w[...]).astype(bf16)
    q = dot(x, q_w[...]).astype(bf16)
    for h in range(q.shape[1] // HEAD_DIM):
        qs[h * n : (h + 1) * n, :] = q[:, h * HEAD_DIM : (h + 1) * HEAD_DIM]
    both = dot(x, conv_w[...]).astype(bf16).astype(f32)
    b = (both[:, 0:ch] * jax.nn.sigmoid(both[:, ch:])).astype(bf16)
    blend[...] = b
    head = b[n - 32 : n - 16, :].astype(f32)
    row = lax.broadcasted_iota(jnp.int32, head.shape, 0)
    offs = off[...].astype(f32)
    for h in range(off.shape[0]):
        head = jnp.where(row == h, offs[h : h + 1, :], head)
    pay[n:, 0:kv] = head.astype(bf16)
    pay[n:, kv:] = b[n - 16 :, :]


def conv_kernel(p1, p3, p7, blend, taps, field, stats, wide):
    n = blend.shape[0]
    half = p1.shape[1] // 2
    reach = taps.shape[0] - 1
    me = lax.axis_index("sp")
    flip = me ^ (me - 1)
    halo = jnp.where(flip == 1, p1[n:, :], jnp.where(flip == 3, p3[n:, :], p7[n:, :]))
    halo = jnp.where(me > 0, halo.astype(f32), 0.0)
    wide[0:16, :] = halo[:, 0:half]
    wide[16:32, :] = halo[:, half:]
    convolve(blend, taps, field, stats, wide)


def conv_plain_kernel(halo, blend, taps, field, stats, wide):
    wide[0:32, :] = halo[...].astype(f32)
    convolve(blend, taps, field, stats, wide)


def convolve(blend, taps, field, stats, wide):
    n = blend.shape[0]
    reach = taps.shape[0] - 1
    wide[32 : 32 + n, :] = blend[...].astype(f32)
    base = 32 - reach
    f = taps[0:1, :] * wide[base : base + n, :]
    for t in range(1, reach + 1):
        f = f + taps[t : t + 1, :] * wide[base + t : base + t + n, :]
    field[...] = f
    ch = f.shape[1]
    mean = jnp.sum(f, axis=1, keepdims=True) / ch
    d = f - mean
    m2 = jnp.sum(d * d, axis=1, keepdims=True)
    stats[0:1, :] = jnp.transpose(jnp.broadcast_to(mean, (n, 128)))[0:1, :]
    stats[1:2, :] = jnp.transpose(jnp.broadcast_to(m2, (n, 128)))[0:1, :]


def shares(q, pays, own, n, per, tri):
    scale = LOG2E * HEAD_DIM ** (-0.5)
    takes, splits, outs = [], [], []
    for pay, mine in zip(pays, own):
        s = lax.dot_general(
            q, pay[0:n, 0:HEAD_DIM], (((1,), (1,)), ((), ())), preferred_element_type=f32
        )
        off = pay[n : n + 16, 0:HEAD_DIM].astype(f32) * LOG2E
        shift = [jnp.broadcast_to(off[h : h + 1, :], (n, n)) for h in range(per)]
        u = s * scale + jnp.concatenate(shift, axis=0)
        soft = jnp.log2(1.0 + jnp.exp2(-jnp.abs(u)))
        take = jnp.minimum(u, 0.0) - soft
        keep = take - u
        if mine:
            keep = jnp.where(before(u.shape, n), keep, 0.0)
        hi = keep.astype(bf16)
        lo = (keep - hi.astype(f32)).astype(bf16)
        takes.append(take)
        splits.append(jnp.concatenate([hi, lo], axis=1))
    for pay, mine, take, split in zip(pays, own, takes, splits):
        sums = dot(split, tri)
        w = jnp.exp2(take + sums[:, 0:n])
        if mine:
            w = jnp.where(before(w.shape, n), w, 0.0)
        outs.append((w.astype(bf16), sums[:, n : 2 * n]))
    return [
        (dot(w, pay[0:n, HEAD_DIM : 2 * HEAD_DIM]), total)
        for pay, (w, total) in zip(pays, outs)
    ]


def before(shape, n):
    row = lax.broadcasted_iota(jnp.int32, shape, 0) & (n - 1)
    return lax.broadcasted_iota(jnp.int32, shape, 1) < row


def tri_of(n):
    r = lax.broadcasted_iota(jnp.int32, (2 * n, 2 * n), 0) & (n - 1)
    c = lax.broadcasted_iota(jnp.int32, (2 * n, 2 * n), 1)
    return jnp.where((r > c) | (c >= n), 1.0, 0.0).astype(bf16)


def normed_heads(att, s_gain, mix, n, per):
    ms = jnp.mean(att * att, axis=1, keepdims=True)
    normed = att * lax.rsqrt(ms + norm_eps)
    for h in range(per):
        part = normed[h * n : (h + 1) * n, :] * s_gain[h : h + 1, :]
        mix[:, h * HEAD_DIM : (h + 1) * HEAD_DIM] = part.astype(bf16)


def by_slot(mix, n, members):
    me = lax.axis_index("tp")
    rows = n // members
    picks = [mix[pl.ds(pl.multiple_of((me ^ k) * rows, rows), rows), :] for k in (0, 2, 1, 3)]
    return jnp.concatenate(picks, axis=0)


def parts_kernel(*refs, slots, blocks, n, per):
    q_ref = refs[0]
    pays = refs[1 : 1 + len(slots)]
    sums = refs[-1]
    me = lax.axis_index("sp")
    found = shares(q_ref[...], pays, [k == 0 for k in slots], n, per, tri_of(n))
    for k, (part, total) in zip(slots, found):
        j = me ^ k
        if k:
            part = jnp.where(j < me, part, 0.0)
            total = jnp.where(j < me, total, 0.0)
        sums[pl.ds(j, 1)] = part[None]
        sums[pl.ds(blocks + j, 1)] = total[None]


def stick_kernel(q_ref, *refs, slots, blocks, members, n, per):
    pays = refs[: len(slots)]
    s_gain, out_w, _, stick, sums, mix = refs[len(slots) :]
    me = lax.axis_index("sp")
    late = shares(q_ref[...], pays, [False] * len(slots), n, per, tri_of(n))
    for k, (part, total) in zip(slots, late):
        j = me ^ k
        sums[pl.ds(j, 1)] = jnp.where(j < me, part, 0.0)[None]
        sums[pl.ds(blocks + j, 1)] = jnp.where(j < me, total, 0.0)[None]
    att = sums[blocks - 1]
    carry = sums[2 * blocks - 1]
    for j in range(blocks - 2, -1, -1):
        att = att + jnp.exp2(carry) * sums[j]
        if j:
            carry = carry + sums[blocks + j]
    normed_heads(att, s_gain, mix, n, per)
    ch = out_w.shape[0] - per * HEAD_DIM
    stick[...] = dot(by_slot(mix, n, members), out_w[ch:, :])


def stick_loop_kernel(q_ref, pays, s_gain, out_w, stick, mix, *, members, n, per):
    me = lax.axis_index("sp")
    q = q_ref[...]
    tri = tri_of(n)

    def step(turn, carried):
        att, carry = carried
        ((part, total),) = shares(q, [pays.at[me - turn]], [False], n, per, tri)
        return att + jnp.exp2(carry) * part, carry + total

    (start,) = shares(q, [pays.at[me]], [True], n, per, tri)
    att, _ = lax.fori_loop(1, me + 1, step, start)
    normed_heads(att, s_gain, mix, n, per)
    ch = out_w.shape[0] - per * HEAD_DIM
    stick[...] = dot(by_slot(mix, n, members), out_w[ch:, :])


def finish_kernel(field, s0, s1, s2, s3, c_gain, out_w, stick, mine, other, send, mix, *, members):
    n, ch = field.shape
    stats = (s0, s1, s2, s3)
    mean = sum(st[0:1, :] for st in stats) / members
    m2 = sum(st[1:2, :] for st in stats)
    m2 = m2 + ch * sum((st[0:1, :] - mean) ** 2 for st in stats)
    rstd = lax.rsqrt(m2 / (ch * members) + norm_eps)
    mean_c = jnp.transpose(jnp.broadcast_to(mean, (ch, n)))
    rstd_c = jnp.transpose(jnp.broadcast_to(rstd, (ch, n)))
    z = (field[...] - mean_c) * rstd_c * c_gain[...]
    mix[...] = (z * jax.nn.sigmoid(z)).astype(bf16)
    out = dot(by_slot(mix, n, members), out_w[0:ch, :]) + stick[...]
    rows = n // members
    mine[...] = out[0:rows, :]
    other[...] = out[rows : 2 * rows, :]
    send[...] = out[2 * rows :, :].astype(bf16)


def call(body, outs, args, scratch=(), flops=0, spaces=None, limit=2**22, aliases={}):
    in_vmem = pl.BlockSpec(memory_space=pltpu.VMEM)
    if spaces is None:
        spaces = [True] * len(args)
    args = [
        pltpu.with_memory_space_constraint(arg, pltpu.VMEM) if held else arg
        for arg, held in zip(args, spaces)
    ]
    return pl.pallas_call(
        body,
        out_shape=[pltpu.VMEM(shape, dtype) for shape, dtype in outs],
        in_specs=[in_vmem] * len(args),
        out_specs=[in_vmem] * len(outs),
        scratch_shapes=scratch,
        input_output_aliases=aliases,
        name=getattr(body, "func", body).__name__,
        cost_estimate=pl.CostEstimate(flops=flops, transcendentals=0, bytes_accessed=0),
        compiler_params=pltpu.CompilerParams(vmem_limit_bytes=limit),
    )(*args)


def shards(
    tokens,
    conv_input,
    conv_gate,
    query_weight,
    key_weight,
    value_weight,
    conv_taps,
    conv_gain,
    key_offsets,
    stick_gain,
    conv_output,
    stick_output,
):
    members = lax.axis_size("tp")
    blocks = lax.axis_size("sp")
    rows, width = tokens.shape
    n = rows * members
    ch = conv_input.shape[1]
    kv = key_weight.shape[1]
    query_cols = query_weight.shape[1]
    per = query_cols // kv
    off = jnp.transpose(key_offsets)
    by_core = swap(tokens, "tp", 1)
    by_chip = swap(tokens, "tp", 2)
    in_vmem = pl.BlockSpec(memory_space=pltpu.VMEM)
    sources = [
        tokens, conv_input, conv_gate, query_weight, key_weight, value_weight, conv_taps,
        conv_gain.reshape(1, ch), off, stick_gain.reshape(per, HEAD_DIM),
        conv_output, stick_output,
    ]
    tok, conv_w, q_w, kv_w, taps, c_gain, off, s_gain, out_w = pl.pallas_call(
        load_kernel,
        out_shape=[
            pltpu.VMEM(shape, dtype)
            for shape, dtype in (
                ((rows, width), bf16),
                ((width, 2 * ch), bf16),
                ((width, query_cols), bf16),
                ((width, 2 * kv), bf16),
                (conv_taps.shape, f32),
                ((1, ch), f32),
                ((per, n), bf16),
                ((per, HEAD_DIM), f32),
                ((ch + query_cols, width), bf16),
            )
        ],
        in_specs=[pl.BlockSpec(memory_space=pltpu.HBM)] * 12,
        out_specs=[in_vmem] * 9,
        scratch_shapes=[pltpu.SemaphoreType.DMA((12,))],
        cost_estimate=pl.CostEstimate(flops=10**9, transcendentals=0, bytes_accessed=5 * 10**6),
        compiler_params=pltpu.CompilerParams(vmem_limit_bytes=2**21),
    )(*[pltpu.with_memory_space_constraint(source, pltpu.HBM) for source in sources])
    by_chip, tok = lax.optimization_barrier((by_chip, tok))
    by_both = swap(by_chip, "tp", 1)
    pay, qs, blend = call(
        project_kernel,
        [((n + 16, 2 * kv), bf16), ((per * n, HEAD_DIM), bf16), ((n, ch), bf16)],
        [tok, by_core, by_chip, by_both, conv_w, q_w, kv_w, off],
        scratch=[pltpu.VMEM((n, width), bf16)],
        flops=2 * n * width * (2 * ch + 4 * kv),
    )
    field_shapes = [((n, ch), f32), ((8, n), f32)]
    wide = [pltpu.VMEM((n + 32, ch), f32)]
    sizes = dict(n=n, per=per)
    heads = per * n
    mixed = [pltpu.VMEM((n, query_cols), bf16)]
    block_flops = 2 * heads * n * HEAD_DIM * 8
    if blocks == 8:
        z2 = swap(pay, "sp", 2)
        z6 = swap(pay, "sp", 6)
        z4 = swap(pay, "sp", 4)
        x1 = swap(pay, "sp", 1)
        x7 = swap(z6, "sp", 1)
        x3 = swap(z2, "sp", 1)
        x5 = swap(z4, "sp", 1)

        def parts(slots, pays, sums):
            args = [qs, *pays] + ([] if sums is None else [sums])
            (out,) = call(
                functools.partial(parts_kernel, slots=slots, blocks=blocks, **sizes),
                [((2 * blocks, heads, HEAD_DIM), f32)],
                args,
                flops=len(slots) * block_flops,
                aliases={} if sums is None else {len(args) - 1: 0},
            )
            return out

        sums = parts((0, 2, 6, 1, 4), (pay, z2, z6, x1, z4), None)
        conv_args = [x1, x3, x7, blend, taps]
        field, stats = call(conv_kernel, field_shapes, conv_args, wide, 64 * n * ch)
        all_stats = [stats] + [swap(stats, "tp", k) for k in (2, 3, 1)]
        body = functools.partial(
            stick_kernel, slots=(3, 7, 5), blocks=blocks, members=members, **sizes
        )
        stick_args = [qs, x3, x7, x5, s_gain, out_w, sums]
        stick_outs = [((2 * blocks, heads, HEAD_DIM), f32)]
        aliases = {6: 1}
        spaces = None
    else:
        pays = lax.all_gather(pay, "sp", axis=0)
        halo = from_behind(blend[n - 32 :], "sp", 1)
        field, stats = call(
            conv_plain_kernel, field_shapes, [halo, blend, taps], wide, 64 * n * ch
        )
        all_stats = [stats] + [swap(stats, "tp", k) for k in (2, 3, 1)]
        body = functools.partial(stick_loop_kernel, members=members, **sizes)
        stick_args = [qs, pays, s_gain, out_w]
        stick_outs = []
        aliases = {}
        spaces = [True, False, True, True]
    stick, *_ = call(
        body,
        [((n, width), f32)] + stick_outs,
        stick_args,
        scratch=mixed,
        flops=block_flops + 2 * n * width * query_cols,
        spaces=spaces,
        aliases=aliases,
        limit=2**22 if blocks == 8 else 2**25,
    )
    mine, other, send = call(
        functools.partial(finish_kernel, members=members),
        [((rows, width), f32), ((rows, width), f32), ((2 * rows, width), bf16)],
        [field, *all_stats, c_gain, out_w, stick],
        scratch=[pltpu.VMEM((n, ch), bf16)],
        flops=2 * n * width * ch,
    )
    got = swap(send, "tp", 1).astype(f32)
    chip = swap((other + got[rows:]).astype(bf16), "tp", 2)
    return (mine + got[:rows] + chip.astype(f32)).astype(bf16)


def solution(mesh):
    return jax.shard_map(
        shards,
        mesh=mesh,
        in_specs=(
            P(("sp", "tp"), None),
            P(None, "tp"),
            P(None, "tp"),
            P(None, "tp"),
            P(None, "tp"),
            P(None, "tp"),
            P(None, "tp"),
            P("tp"),
            P("sp", "tp"),
            P("tp"),
            P("tp", None),
            P("tp", None),
        ),
        out_specs=P(("sp", "tp"), None),
        check_vma=False,
    )
```

```python
import functools

import jax
import jax.numpy as jnp
from jax import lax
from jax.experimental import pallas as pl
from jax.experimental.pallas import tpu as pltpu
from jax.sharding import PartitionSpec as P


HEAD_DIM = 128
LOG2E = 1.4426950408889634
norm_eps = 1e-05
f32 = jnp.float32
bf16 = jnp.bfloat16


def swap(value, axis, by):
    count = lax.axis_size(axis)
    return lax.ppermute(value, axis, [(i, i ^ by) for i in range(count)])


def from_behind(value, axis, by):
    count = lax.axis_size(axis)
    pairs = [(i, i + by) for i in range(count) if 0 <= i + by < count]
    return lax.ppermute(value, axis, pairs)


def dot(a, b):
    return jnp.dot(a, b, preferred_element_type=f32)


def load_kernel(*refs):
    sources, sems = refs[:12], refs[-1]
    tokens, w_in, w_gate, w_q, w_k, w_v, taps, c_gain, off, s_gain, w_c, w_s = sources
    tok, conv_w, q_w, kv_w, taps_v, c_gain_v, off_v, s_gain_v, out_w = refs[12:-1]
    ch = w_in.shape[1]
    kv = w_k.shape[1]
    pairs = [
        (w_k, kv_w.at[:, 0:kv]),
        (w_v, kv_w.at[:, kv:]),
        (w_q, q_w),
        (w_in, conv_w.at[:, 0:ch]),
        (w_gate, conv_w.at[:, ch:]),
        (tokens, tok),
        (taps, taps_v),
        (c_gain, c_gain_v),
        (off, off_v),
        (s_gain, s_gain_v),
        (w_c, out_w.at[0:ch]),
        (w_s, out_w.at[ch:]),
    ]
    copies = [pltpu.make_async_copy(a, b, sems.at[i]) for i, (a, b) in enumerate(pairs)]
    for copy in copies:
        copy.start()
    for copy in copies:
        copy.wait()


def project_kernel(t0, t1, t2, t3, conv_w, q_w, kv_w, off, pay, pay_x, qs, blend, tail, x_all):
    rows = t0.shape[0]
    me = lax.axis_index("tp")
    for k, t in enumerate((t0, t1, t2, t3)):
        x_all[pl.ds(pl.multiple_of((me ^ k) * rows, rows), rows), :] = t[...]
    x = x_all[...]
    n = x.shape[0]
    ch = conv_w.shape[1] // 2
    kv = kv_w.shape[1] // 2
    rows_kv = dot(x, kv_w[...]).astype(bf16)
    pay[0:n, :] = rows_kv
    pay_x[0:n, :] = rows_kv
    q = dot(x, q_w[...]).astype(bf16)
    for h in range(q.shape[1] // HEAD_DIM):
        qs[h * n : (h + 1) * n, :] = q[:, h * HEAD_DIM : (h + 1) * HEAD_DIM]
    both = dot(x, conv_w[...]).astype(bf16).astype(f32)
    b = (both[:, 0:ch] * jax.nn.sigmoid(both[:, ch:])).astype(bf16)
    blend[...] = b
    tail[...] = b[n - tail.shape[0] :, :]
    row = lax.broadcasted_iota(jnp.int32, (8, kv), 0)
    offs = off[...].astype(f32)
    head = jnp.zeros((8, kv), f32)
    for h in range(off.shape[0]):
        head = jnp.where(row == h, offs[h : h + 1, :], head)
    for out in (pay, pay_x):
        out[n : n + 8, 0:kv] = head.astype(bf16)
        out[n : n + 8, kv:] = jnp.zeros((8, kv), bf16)
    pay_x[n + 8 :, 0:kv] = b[n - 32 : n - 16, :]
    pay_x[n + 8 :, kv:] = b[n - 16 :, :]


def conv_kernel(even, odd, blend, taps, field, stats, wide):
    n = blend.shape[0]
    kv = odd.shape[1] // 2
    me = lax.axis_index("sp")
    right = me & 1 == 1
    for half in (0, 1):
        fill = odd[n + 8 :, half * kv : (half + 1) * kv].astype(f32)
        rest = jnp.where(me > 0, even[16 * half : 16 * half + 16, :].astype(f32), 0.0)
        wide[16 * half : 16 * half + 16, :] = jnp.where(right, fill, rest)
    convolve(blend, taps, field, stats, wide)


def conv_plain_kernel(halo, blend, taps, field, stats, wide):
    wide[0:32, :] = halo[...].astype(f32)
    convolve(blend, taps, field, stats, wide)


def convolve(blend, taps, field, stats, wide):
    n = blend.shape[0]
    reach = taps.shape[0] - 1
    wide[32 : 32 + n, :] = blend[...].astype(f32)
    base = 32 - reach
    f = taps[0:1, :] * wide[base : base + n, :]
    for t in range(1, reach + 1):
        f = f + taps[t : t + 1, :] * wide[base + t : base + t + n, :]
    field[...] = f
    ch = f.shape[1]
    mean = jnp.sum(f, axis=1, keepdims=True) / ch
    d = f - mean
    m2 = jnp.sum(d * d, axis=1, keepdims=True)
    stats[0:1, :] = jnp.transpose(jnp.broadcast_to(mean, (n, 128)))[0:1, :]
    stats[1:2, :] = jnp.transpose(jnp.broadcast_to(m2, (n, 128)))[0:1, :]


def both_stats(a, b, count):
    gap = a[0:1, :] - b[0:1, :]
    return (a[0:1, :] + b[0:1, :]) / 2, a[1:2, :] + b[1:2, :] + gap * gap * (count / 2)


def pair_kernel(stats, peer, out, *, ch):
    out[0:1, :], out[1:2, :] = both_stats(stats, peer, ch)


def join_kernel(za, zb, joined):
    joined[0] = za[...]
    joined[1] = zb[...]


def shares(q, pays, own, n, per, tri):
    scale = LOG2E * HEAD_DIM ** (-0.5)
    takes, splits, outs = [], [], []
    for pay, mine in zip(pays, own):
        s = lax.dot_general(
            q, pay[0:n, 0:HEAD_DIM], (((1,), (1,)), ((), ())), preferred_element_type=f32
        )
        off = pay[n : n + 8, 0:HEAD_DIM].astype(f32) * LOG2E
        shift = [jnp.broadcast_to(off[h : h + 1, :], (n, n)) for h in range(per)]
        u = s * scale + jnp.concatenate(shift, axis=0)
        soft = jnp.log2(1.0 + jnp.exp2(-jnp.abs(u)))
        take = jnp.minimum(u, 0.0) - soft
        keep = take - u
        if mine:
            keep = jnp.where(before(u.shape, n), keep, 0.0)
        hi = keep.astype(bf16)
        lo = (keep - hi.astype(f32)).astype(bf16)
        takes.append(take)
        splits.append(jnp.concatenate([hi, lo], axis=1))
    for pay, mine, take, split in zip(pays, own, takes, splits):
        sums = dot(split, tri)
        w = jnp.exp2(take + sums[:, 0:n])
        if mine:
            w = jnp.where(before(w.shape, n), w, 0.0)
        outs.append((w.astype(bf16), sums[:, n : 2 * n]))
    return [
        (dot(w, pay[0:n, HEAD_DIM : 2 * HEAD_DIM]), total)
        for pay, (w, total) in zip(pays, outs)
    ]


def before(shape, n):
    row = lax.broadcasted_iota(jnp.int32, shape, 0) & (n - 1)
    return lax.broadcasted_iota(jnp.int32, shape, 1) < row


def tri_of(n):
    r = lax.broadcasted_iota(jnp.int32, (2 * n, 2 * n), 0) & (n - 1)
    c = lax.broadcasted_iota(jnp.int32, (2 * n, 2 * n), 1)
    return jnp.where((r > c) | (c >= n), 1.0, 0.0).astype(bf16)


def normed_heads(att, s_gain, mix, n, per):
    ms = jnp.mean(att * att, axis=1, keepdims=True)
    normed = att * lax.rsqrt(ms + norm_eps)
    for h in range(per):
        part = normed[h * n : (h + 1) * n, :] * s_gain[h : h + 1, :]
        mix[:, h * HEAD_DIM : (h + 1) * HEAD_DIM] = part.astype(bf16)


def by_slot(mix, n, members):
    me = lax.axis_index("tp")
    rows = n // members
    picks = [mix[pl.ds(pl.multiple_of((me ^ k) * rows, rows), rows), :] for k in (0, 2, 1, 3)]
    return jnp.concatenate(picks, axis=0)


def parts_kernel(*refs, slots, blocks, n, per):
    q_ref = refs[0]
    pays = views(refs[1:-1])
    sums = refs[-1]
    me = lax.axis_index("sp")
    found = shares(q_ref[...], pays, [k == 0 for k in slots], n, per, tri_of(n))
    for k, (part, total) in zip(slots, found):
        j = me ^ k
        if k:
            part = jnp.where(j < me, part, 0.0)
            total = jnp.where(j < me, total, 0.0)
        sums[pl.ds(j, 1)] = part[None]
        sums[pl.ds(blocks + j, 1)] = total[None]


def views(refs):
    flat = []
    for ref in refs:
        flat += [ref] if len(ref.shape) == 2 else [ref.at[i] for i in range(ref.shape[0])]
    return flat


def stick_kernel(q_ref, *refs, slots, blocks, members, n, per):
    s_gain, out_w, _, stick, sums, mix = refs[-6:]
    pays = views(refs[:-6])
    me = lax.axis_index("sp")
    late = shares(q_ref[...], pays, [False] * len(slots), n, per, tri_of(n))
    for k, (part, total) in zip(slots, late):
        j = me ^ k
        sums[pl.ds(j, 1)] = jnp.where(j < me, part, 0.0)[None]
        sums[pl.ds(blocks + j, 1)] = jnp.where(j < me, total, 0.0)[None]
    att = sums[blocks - 1]
    carry = sums[2 * blocks - 1]
    for j in range(blocks - 2, -1, -1):
        att = att + jnp.exp2(carry) * sums[j]
        if j:
            carry = carry + sums[blocks + j]
    normed_heads(att, s_gain, mix, n, per)
    ch = out_w.shape[0] - per * HEAD_DIM
    stick[...] = dot(by_slot(mix, n, members), out_w[ch:, :])


def stick_loop_kernel(q_ref, pays, s_gain, out_w, stick, mix, *, members, n, per):
    me = lax.axis_index("sp")
    q = q_ref[...]
    tri = tri_of(n)

    def step(turn, carried):
        att, carry = carried
        ((part, total),) = shares(q, [pays.at[me - turn]], [False], n, per, tri)
        return att + jnp.exp2(carry) * part, carry + total

    (start,) = shares(q, [pays.at[me]], [True], n, per, tri)
    att, _ = lax.fori_loop(1, me + 1, step, start)
    normed_heads(att, s_gain, mix, n, per)
    ch = out_w.shape[0] - per * HEAD_DIM
    stick[...] = dot(by_slot(mix, n, members), out_w[ch:, :])


def finish_kernel(field, near, far, c_gain, out_w, stick, mine, other, send, mix, *, members):
    n, ch = field.shape
    mean, m2 = both_stats(near, far, ch * members // 2)
    rstd = lax.rsqrt(m2 / (ch * members) + norm_eps)
    mean_c = jnp.transpose(jnp.broadcast_to(mean, (ch, n)))
    rstd_c = jnp.transpose(jnp.broadcast_to(rstd, (ch, n)))
    z = (field[...] - mean_c) * rstd_c * c_gain[...]
    mix[...] = (z * jax.nn.sigmoid(z)).astype(bf16)
    out = dot(by_slot(mix, n, members), out_w[0:ch, :]) + stick[...]
    rows = n // members
    mine[...] = out[0:rows, :]
    other[...] = out[rows : 2 * rows, :]
    send[...] = out[2 * rows :, :].astype(bf16)


def call(body, outs, args, scratch=(), flops=0, spaces=None, limit=2**22, aliases={}):
    in_vmem = pl.BlockSpec(memory_space=pltpu.VMEM)
    if spaces is None:
        spaces = [True] * len(args)
    args = [
        pltpu.with_memory_space_constraint(arg, pltpu.VMEM) if held else arg
        for arg, held in zip(args, spaces)
    ]
    return pl.pallas_call(
        body,
        out_shape=[pltpu.VMEM(shape, dtype) for shape, dtype in outs],
        in_specs=[in_vmem] * len(args),
        out_specs=[in_vmem] * len(outs),
        scratch_shapes=scratch,
        input_output_aliases=aliases,
        cost_estimate=pl.CostEstimate(flops=flops, transcendentals=0, bytes_accessed=0),
        compiler_params=pltpu.CompilerParams(vmem_limit_bytes=limit),
    )(*args)


def shards(
    tokens,
    conv_input,
    conv_gate,
    query_weight,
    key_weight,
    value_weight,
    conv_taps,
    conv_gain,
    key_offsets,
    stick_gain,
    conv_output,
    stick_output,
):
    members = lax.axis_size("tp")
    blocks = lax.axis_size("sp")
    rows, width = tokens.shape
    n = rows * members
    ch = conv_input.shape[1]
    kv = key_weight.shape[1]
    query_cols = query_weight.shape[1]
    per = query_cols // kv
    off = jnp.transpose(key_offsets)
    by_core = swap(tokens, "tp", 1)
    by_chip = swap(tokens, "tp", 2)
    in_vmem = pl.BlockSpec(memory_space=pltpu.VMEM)
    sources = [
        tokens, conv_input, conv_gate, query_weight, key_weight, value_weight, conv_taps,
        conv_gain.reshape(1, ch), off, stick_gain.reshape(per, HEAD_DIM),
        conv_output, stick_output,
    ]
    tok, conv_w, q_w, kv_w, taps, c_gain, off, s_gain, out_w = pl.pallas_call(
        load_kernel,
        out_shape=[
            pltpu.VMEM(shape, dtype)
            for shape, dtype in (
                ((rows, width), bf16),
                ((width, 2 * ch), bf16),
                ((width, query_cols), bf16),
                ((width, 2 * kv), bf16),
                (conv_taps.shape, f32),
                ((1, ch), f32),
                ((per, n), bf16),
                ((per, HEAD_DIM), f32),
                ((ch + query_cols, width), bf16),
            )
        ],
        in_specs=[pl.BlockSpec(memory_space=pltpu.HBM)] * 12,
        out_specs=[in_vmem] * 9,
        scratch_shapes=[pltpu.SemaphoreType.DMA((12,))],
        cost_estimate=pl.CostEstimate(flops=10**9, transcendentals=0, bytes_accessed=5 * 10**6),
        compiler_params=pltpu.CompilerParams(vmem_limit_bytes=2**21),
    )(*[pltpu.with_memory_space_constraint(source, pltpu.HBM) for source in sources])
    by_chip, tok = lax.optimization_barrier((by_chip, tok))
    by_both = swap(by_chip, "tp", 1)
    pay, pay_x, qs, blend, tail = call(
        project_kernel,
        [
            ((n + 8, 2 * kv), bf16),
            ((n + 24, 2 * kv), bf16),
            ((per * n, HEAD_DIM), bf16),
            ((n, ch), bf16),
            ((32, ch), bf16),
        ],
        [tok, by_core, by_chip, by_both, conv_w, q_w, kv_w, off],
        scratch=[pltpu.VMEM((n, width), bf16)],
        flops=2 * n * width * (2 * ch + 4 * kv),
    )
    sizes = dict(n=n, per=per)
    heads = per * n
    mixed = [pltpu.VMEM((n, query_cols), bf16)]
    block_flops = 2 * heads * n * HEAD_DIM * 8
    stat = ((8, n), f32)
    if blocks == 8:
        z2 = swap(pay, "sp", 2)
        z6 = swap(pay, "sp", 6)
        z4 = swap(pay, "sp", 4)
        x1 = swap(pay_x, "sp", 1)
        x3 = swap(z2, "sp", 1)
        pairs = []
        for i in range(1, blocks - 1, 2):
            pairs += [(i, i + 1), (i + 1, i)]
        even = lax.ppermute(tail, "sp", pairs)
        conv_body = conv_kernel
        conv_args = [even, x1, blend, taps]
    else:
        pays = lax.all_gather(pay, "sp", axis=0)
        conv_body = conv_plain_kernel
        conv_args = [from_behind(tail, "sp", 1), blend, taps]
    field, stats = call(
        conv_body,
        [((n, ch), f32), stat],
        conv_args,
        [pltpu.VMEM((n + 32, ch), f32)],
        64 * n * ch,
    )
    peer = swap(stats, "tp", 1)
    (near,) = call(functools.partial(pair_kernel, ch=ch), [stat], [stats, peer])
    if blocks == 8:
        (z46,) = call(join_kernel, [((2, n + 8, 2 * kv), bf16)], [z4, z6])
        x57 = swap(z46, "sp", 1)
        (sums,) = call(
            functools.partial(parts_kernel, slots=(0, 2, 1, 4, 6), blocks=blocks, **sizes),
            [((2 * blocks, heads, HEAD_DIM), f32)],
            [qs, pay, z2, x1, z46],
            flops=5 * block_flops,
        )
        body = functools.partial(
            stick_kernel, slots=(3, 5, 7), blocks=blocks, members=members, **sizes
        )
        stick_args = [qs, x3, x57, s_gain, out_w, sums]
        stick_outs = [((2 * blocks, heads, HEAD_DIM), f32)]
        aliases = {5: 1}
        spaces = None
    else:
        body = functools.partial(stick_loop_kernel, members=members, **sizes)
        stick_args = [qs, pays, s_gain, out_w]
        stick_outs = []
        aliases = {}
        spaces = [True, False, True, True]
    far = swap(near, "tp", 2)
    stick, *_ = call(
        body,
        [((n, width), f32)] + stick_outs,
        stick_args,
        scratch=mixed,
        flops=block_flops + 2 * n * width * query_cols,
        spaces=spaces,
        aliases=aliases,
        limit=2**22 if blocks == 8 else 2**25,
    )
    mine, other, send = call(
        functools.partial(finish_kernel, members=members),
        [((rows, width), f32), ((rows, width), f32), ((2 * rows, width), bf16)],
        [field, near, far, c_gain, out_w, stick],
        scratch=[pltpu.VMEM((n, ch), bf16)],
        flops=2 * n * width * ch,
    )
    got = swap(send, "tp", 1).astype(f32)
    chip = swap((other + got[rows:]).astype(bf16), "tp", 2)
    return (mine + got[:rows] + chip.astype(f32)).astype(bf16)


def solution(mesh):
    return jax.shard_map(
        shards,
        mesh=mesh,
        in_specs=(
            P(("sp", "tp"), None),
            P(None, "tp"),
            P(None, "tp"),
            P(None, "tp"),
            P(None, "tp"),
            P(None, "tp"),
            P(None, "tp"),
            P("tp"),
            P("sp", "tp"),
            P("tp"),
            P("tp", None),
            P("tp", None),
        ),
        out_specs=P(("sp", "tp"), None),
        check_vma=False,
    )
```

```python
import functools

import jax
import jax.numpy as jnp
from jax import lax
from jax.experimental import pallas as pl
from jax.experimental.pallas import tpu as pltpu
from jax.sharding import PartitionSpec as P


HEAD_DIM = 128
LOG2E = 1.4426950408889634
norm_eps = 1e-05
f32 = jnp.float32
bf16 = jnp.bfloat16


def swap(value, axis, by):
    count = lax.axis_size(axis)
    return lax.ppermute(value, axis, [(i, i ^ by) for i in range(count)])


def from_behind(value, axis, by):
    count = lax.axis_size(axis)
    pairs = [(i, i + by) for i in range(count) if 0 <= i + by < count]
    return lax.ppermute(value, axis, pairs)


def dot(a, b):
    return jnp.dot(a, b, preferred_element_type=f32)


def load_kernel(*refs):
    sources, sems = refs[:12], refs[-1]
    tokens, w_in, w_gate, w_q, w_k, w_v, taps, c_gain, off, s_gain, w_c, w_s = sources
    tok, conv_w, q_w, kv_w, taps_v, c_gain_v, off_v, s_gain_v, out_w = refs[12:-1]
    ch = w_in.shape[1]
    kv = w_k.shape[1]
    pairs = [
        (w_k, kv_w.at[:, 0:kv]),
        (w_v, kv_w.at[:, kv:]),
        (w_q, q_w),
        (w_in, conv_w.at[:, 0:ch]),
        (w_gate, conv_w.at[:, ch:]),
        (tokens, tok),
        (taps, taps_v),
        (c_gain, c_gain_v),
        (off, off_v),
        (s_gain, s_gain_v),
        (w_c, out_w.at[0:ch]),
        (w_s, out_w.at[ch:]),
    ]
    copies = [pltpu.make_async_copy(a, b, sems.at[i]) for i, (a, b) in enumerate(pairs)]
    for copy in copies:
        copy.start()
    for copy in copies:
        copy.wait()


def keys_kernel(t0, t1, t2, t3, kv_w, off, pay, x_all):
    rows = t0.shape[0]
    me = lax.axis_index("tp")
    for k, t in enumerate((t0, t1, t2, t3)):
        x_all[pl.ds(pl.multiple_of((me ^ k) * rows, rows), rows), :] = t[...]
    n = x_all.shape[0]
    kv = kv_w.shape[1] // 2
    pay[0:n, :] = dot(x_all[...], kv_w[...]).astype(bf16)
    row = lax.broadcasted_iota(jnp.int32, (8, kv), 0)
    offs = off[...].astype(f32)
    head = jnp.zeros((8, kv), f32)
    for h in range(off.shape[0]):
        head = jnp.where(row == h, offs[h : h + 1, :], head)
    pay[n:, 0:kv] = head.astype(bf16)
    pay[n:, kv:] = jnp.zeros((8, kv), bf16)


def project_kernel(x_all, conv_w, q_w, pay, pay_x, qs, blend, tail):
    x = x_all[...]
    n = x.shape[0]
    ch = conv_w.shape[1] // 2
    kv = pay.shape[1] // 2
    both = dot(x, conv_w[...]).astype(bf16).astype(f32)
    q = dot(x, q_w[...]).astype(bf16)
    for h in range(q.shape[1] // HEAD_DIM):
        qs[h * n : (h + 1) * n, :] = q[:, h * HEAD_DIM : (h + 1) * HEAD_DIM]
    b = (both[:, 0:ch] * jax.nn.sigmoid(both[:, ch:])).astype(bf16)
    blend[...] = b
    tail[...] = b[n - tail.shape[0] :, :]
    pay_x[0 : n + 8, :] = pay[...]
    pay_x[n + 8 :, 0:kv] = b[n - 32 : n - 16, :]
    pay_x[n + 8 :, kv:] = b[n - 16 :, :]


def conv_kernel(even, odd, blend, taps, field, stats, wide):
    n = blend.shape[0]
    kv = odd.shape[1] // 2
    me = lax.axis_index("sp")
    right = me & 1 == 1
    for half in (0, 1):
        fill = odd[n + 8 :, half * kv : (half + 1) * kv].astype(f32)
        rest = jnp.where(me > 0, even[16 * half : 16 * half + 16, :].astype(f32), 0.0)
        wide[16 * half : 16 * half + 16, :] = jnp.where(right, fill, rest)
    convolve(blend, taps, field, stats, wide)


def conv_plain_kernel(halo, blend, taps, field, stats, wide):
    wide[0:32, :] = halo[...].astype(f32)
    convolve(blend, taps, field, stats, wide)


def convolve(blend, taps, field, stats, wide):
    n = blend.shape[0]
    reach = taps.shape[0] - 1
    wide[32 : 32 + n, :] = blend[...].astype(f32)
    base = 32 - reach
    f = taps[0:1, :] * wide[base : base + n, :]
    for t in range(1, reach + 1):
        f = f + taps[t : t + 1, :] * wide[base + t : base + t + n, :]
    field[...] = f
    ch = f.shape[1]
    mean = jnp.sum(f, axis=1, keepdims=True) / ch
    d = f - mean
    m2 = jnp.sum(d * d, axis=1, keepdims=True)
    stats[0:1, :] = jnp.transpose(jnp.broadcast_to(mean, (n, 128)))[0:1, :]
    stats[1:2, :] = jnp.transpose(jnp.broadcast_to(m2, (n, 128)))[0:1, :]


def both_stats(mean_a, m2_a, mean_b, m2_b, count):
    gap = mean_a - mean_b
    return (mean_a + mean_b) / 2, m2_a + m2_b + gap * gap * (count / 2)


def join_kernel(za, zb, joined):
    joined[0] = za[...]
    joined[1] = zb[...]


def shares(q, pays, own, n, per, tri):
    scale = LOG2E * HEAD_DIM ** (-0.5)
    takes, splits, outs = [], [], []
    for pay, mine in zip(pays, own):
        s = lax.dot_general(
            q, pay[0:n, 0:HEAD_DIM], (((1,), (1,)), ((), ())), preferred_element_type=f32
        )
        off = pay[n : n + 8, 0:HEAD_DIM].astype(f32) * LOG2E
        shift = [jnp.broadcast_to(off[h : h + 1, :], (n, n)) for h in range(per)]
        u = s * scale + jnp.concatenate(shift, axis=0)
        soft = jnp.log2(1.0 + jnp.exp2(-jnp.abs(u)))
        take = jnp.minimum(u, 0.0) - soft
        keep = take - u
        if mine:
            keep = jnp.where(before(u.shape, n), keep, 0.0)
        hi = keep.astype(bf16)
        lo = (keep - hi.astype(f32)).astype(bf16)
        takes.append(take)
        splits.append(jnp.concatenate([hi, lo], axis=1))
    for pay, mine, take, split in zip(pays, own, takes, splits):
        sums = dot(split, tri)
        w = jnp.exp2(take + sums[:, 0:n])
        if mine:
            w = jnp.where(before(w.shape, n), w, 0.0)
        outs.append((w.astype(bf16), sums[:, n : 2 * n]))
    return [
        (dot(w, pay[0:n, HEAD_DIM : 2 * HEAD_DIM]), total)
        for pay, (w, total) in zip(pays, outs)
    ]


def before(shape, n):
    row = lax.broadcasted_iota(jnp.int32, shape, 0) & (n - 1)
    return lax.broadcasted_iota(jnp.int32, shape, 1) < row


def tri_of(n):
    r = lax.broadcasted_iota(jnp.int32, (2 * n, 2 * n), 0) & (n - 1)
    c = lax.broadcasted_iota(jnp.int32, (2 * n, 2 * n), 1)
    return jnp.where((r > c) | (c >= n), 1.0, 0.0).astype(bf16)


def normed_heads(att, s_gain, mix, n, per):
    ms = jnp.mean(att * att, axis=1, keepdims=True)
    normed = att * lax.rsqrt(ms + norm_eps)
    for h in range(per):
        part = normed[h * n : (h + 1) * n, :] * s_gain[h : h + 1, :]
        mix[:, h * HEAD_DIM : (h + 1) * HEAD_DIM] = part.astype(bf16)


def by_slot(mix, n, members):
    me = lax.axis_index("tp")
    rows = n // members
    picks = [mix[pl.ds(pl.multiple_of((me ^ k) * rows, rows), rows), :] for k in (0, 2, 1, 3)]
    return jnp.concatenate(picks, axis=0)


def parts_kernel(*refs, slots, blocks, n, per):
    q_ref = refs[0]
    pays = views(refs[1:-1])
    sums = refs[-1]
    me = lax.axis_index("sp")
    found = shares(q_ref[...], pays, [k == 0 for k in slots], n, per, tri_of(n))
    for k, (part, total) in zip(slots, found):
        j = me ^ k
        if k:
            part = jnp.where(j < me, part, 0.0)
            total = jnp.where(j < me, total, 0.0)
        sums[pl.ds(j, 1)] = part[None]
        sums[pl.ds(blocks + j, 1)] = total[None]


def views(refs):
    flat = []
    for ref in refs:
        flat += [ref] if len(ref.shape) == 2 else [ref.at[i] for i in range(ref.shape[0])]
    return flat


def stick_kernel(q_ref, *refs, slots, blocks, members, n, per):
    s_gain, out_w, _, stick, sums, mix = refs[-6:]
    pays = views(refs[:-6])
    me = lax.axis_index("sp")
    late = shares(q_ref[...], pays, [False] * len(slots), n, per, tri_of(n))
    for k, (part, total) in zip(slots, late):
        j = me ^ k
        sums[pl.ds(j, 1)] = jnp.where(j < me, part, 0.0)[None]
        sums[pl.ds(blocks + j, 1)] = jnp.where(j < me, total, 0.0)[None]
    att = sums[blocks - 1]
    carry = sums[2 * blocks - 1]
    for j in range(blocks - 2, -1, -1):
        att = att + jnp.exp2(carry) * sums[j]
        if j:
            carry = carry + sums[blocks + j]
    normed_heads(att, s_gain, mix, n, per)
    ch = out_w.shape[0] - per * HEAD_DIM
    stick[...] = dot(by_slot(mix, n, members), out_w[ch:, :])


def stick_loop_kernel(q_ref, pays, s_gain, out_w, stick, mix, *, members, n, per):
    me = lax.axis_index("sp")
    q = q_ref[...]
    tri = tri_of(n)

    def step(turn, carried):
        att, carry = carried
        ((part, total),) = shares(q, [pays.at[me - turn]], [False], n, per, tri)
        return att + jnp.exp2(carry) * part, carry + total

    (start,) = shares(q, [pays.at[me]], [True], n, per, tri)
    att, _ = lax.fori_loop(1, me + 1, step, start)
    normed_heads(att, s_gain, mix, n, per)
    ch = out_w.shape[0] - per * HEAD_DIM
    stick[...] = dot(by_slot(mix, n, members), out_w[ch:, :])


def finish_kernel(field, own, core, chip, both, c_gain, out_w, stick, mine, other, send, mix, *, members):
    n, ch = field.shape
    near = both_stats(own[0:1, :], own[1:2, :], core[0:1, :], core[1:2, :], ch)
    far = both_stats(chip[0:1, :], chip[1:2, :], both[0:1, :], both[1:2, :], ch)
    mean, m2 = both_stats(*near, *far, 2 * ch)
    rstd = lax.rsqrt(m2 / (ch * members) + norm_eps)
    mean_c = jnp.transpose(jnp.broadcast_to(mean, (ch, n)))
    rstd_c = jnp.transpose(jnp.broadcast_to(rstd, (ch, n)))
    z = (field[...] - mean_c) * rstd_c * c_gain[...]
    mix[...] = (z * jax.nn.sigmoid(z)).astype(bf16)
    out = dot(by_slot(mix, n, members), out_w[0:ch, :]) + stick[...]
    rows = n // members
    mine[...] = out[0:rows, :]
    other[...] = out[rows : 2 * rows, :]
    send[...] = out[2 * rows :, :].astype(bf16)


def call(body, outs, args, scratch=(), flops=0, spaces=None, limit=2**22, aliases={}):
    in_vmem = pl.BlockSpec(memory_space=pltpu.VMEM)
    if spaces is None:
        spaces = [True] * len(args)
    args = [
        pltpu.with_memory_space_constraint(arg, pltpu.VMEM) if held else arg
        for arg, held in zip(args, spaces)
    ]
    return pl.pallas_call(
        body,
        out_shape=[pltpu.VMEM(shape, dtype) for shape, dtype in outs],
        in_specs=[in_vmem] * len(args),
        out_specs=[in_vmem] * len(outs),
        scratch_shapes=scratch,
        input_output_aliases=aliases,
        cost_estimate=pl.CostEstimate(flops=flops, transcendentals=0, bytes_accessed=0),
        compiler_params=pltpu.CompilerParams(vmem_limit_bytes=limit),
    )(*args)


def shards(
    tokens,
    conv_input,
    conv_gate,
    query_weight,
    key_weight,
    value_weight,
    conv_taps,
    conv_gain,
    key_offsets,
    stick_gain,
    conv_output,
    stick_output,
):
    members = lax.axis_size("tp")
    blocks = lax.axis_size("sp")
    rows, width = tokens.shape
    n = rows * members
    ch = conv_input.shape[1]
    kv = key_weight.shape[1]
    query_cols = query_weight.shape[1]
    per = query_cols // kv
    off = jnp.transpose(key_offsets)
    by_core = swap(tokens, "tp", 1)
    by_chip = swap(tokens, "tp", 2)
    in_vmem = pl.BlockSpec(memory_space=pltpu.VMEM)
    sources = [
        tokens, conv_input, conv_gate, query_weight, key_weight, value_weight, conv_taps,
        conv_gain.reshape(1, ch), off, stick_gain.reshape(per, HEAD_DIM),
        conv_output, stick_output,
    ]
    tok, conv_w, q_w, kv_w, taps, c_gain, off, s_gain, out_w = pl.pallas_call(
        load_kernel,
        out_shape=[
            pltpu.VMEM(shape, dtype)
            for shape, dtype in (
                ((rows, width), bf16),
                ((width, 2 * ch), bf16),
                ((width, query_cols), bf16),
                ((width, 2 * kv), bf16),
                (conv_taps.shape, f32),
                ((1, ch), f32),
                ((per, n), bf16),
                ((per, HEAD_DIM), f32),
                ((ch + query_cols, width), bf16),
            )
        ],
        in_specs=[pl.BlockSpec(memory_space=pltpu.HBM)] * 12,
        out_specs=[in_vmem] * 9,
        scratch_shapes=[pltpu.SemaphoreType.DMA((12,))],
        cost_estimate=pl.CostEstimate(flops=10**9, transcendentals=0, bytes_accessed=5 * 10**6),
        compiler_params=pltpu.CompilerParams(vmem_limit_bytes=2**21),
    )(*[pltpu.with_memory_space_constraint(source, pltpu.HBM) for source in sources])
    by_chip, tok = lax.optimization_barrier((by_chip, tok))
    by_both = swap(by_chip, "tp", 1)
    pay, x_all = call(
        keys_kernel,
        [((n + 8, 2 * kv), bf16), ((n, width), bf16)],
        [tok, by_core, by_chip, by_both, kv_w, off],
        flops=2 * n * width * 2 * kv,
    )
    pay_x, qs, blend, tail = call(
        project_kernel,
        [
            ((n + 24, 2 * kv), bf16),
            ((per * n, HEAD_DIM), bf16),
            ((n, ch), bf16),
            ((32, ch), bf16),
        ],
        [x_all, conv_w, q_w, pay],
        flops=2 * n * width * (2 * ch + query_cols),
    )
    sizes = dict(n=n, per=per)
    heads = per * n
    mixed = [pltpu.VMEM((n, query_cols), bf16)]
    block_flops = 2 * heads * n * HEAD_DIM * 8
    stat = ((8, n), f32)
    if blocks == 8:
        z2 = swap(pay, "sp", 2)
        z6 = swap(pay, "sp", 6)
        z4 = swap(pay, "sp", 4)
        x1 = swap(pay_x, "sp", 1)
        x3 = swap(z2, "sp", 1)
        pairs = []
        for i in range(1, blocks - 1, 2):
            pairs += [(i, i + 1), (i + 1, i)]
        even = lax.ppermute(tail, "sp", pairs)
        conv_body = conv_kernel
        conv_args = [even, x1, blend, taps]
    else:
        pays = lax.all_gather(pay, "sp", axis=0)
        conv_body = conv_plain_kernel
        conv_args = [from_behind(tail, "sp", 1), blend, taps]
    field, stats = call(
        conv_body,
        [((n, ch), f32), stat],
        conv_args,
        [pltpu.VMEM((n + 32, ch), f32)],
        64 * n * ch,
    )
    peer = swap(stats, "tp", 1)
    chip = swap(stats, "tp", 2)
    both = swap(stats, "tp", 3)
    if blocks == 8:
        (z46,) = call(join_kernel, [((2, n + 8, 2 * kv), bf16)], [z4, z6])
        x57 = swap(z46, "sp", 1)
        (sums,) = call(
            functools.partial(parts_kernel, slots=(0, 2, 1, 4, 6), blocks=blocks, **sizes),
            [((2 * blocks, heads, HEAD_DIM), f32)],
            [qs, pay, z2, x1, z46],
            flops=5 * block_flops,
        )
        body = functools.partial(
            stick_kernel, slots=(3, 5, 7), blocks=blocks, members=members, **sizes
        )
        stick_args = [qs, x3, x57, s_gain, out_w, sums]
        stick_outs = [((2 * blocks, heads, HEAD_DIM), f32)]
        aliases = {5: 1}
        spaces = None
    else:
        body = functools.partial(stick_loop_kernel, members=members, **sizes)
        stick_args = [qs, pays, s_gain, out_w]
        stick_outs = []
        aliases = {}
        spaces = [True, False, True, True]
    stick, *_ = call(
        body,
        [((n, width), f32)] + stick_outs,
        stick_args,
        scratch=mixed,
        flops=block_flops + 2 * n * width * query_cols,
        spaces=spaces,
        aliases=aliases,
        limit=2**22 if blocks == 8 else 2**25,
    )
    mine, other, send = call(
        functools.partial(finish_kernel, members=members),
        [((rows, width), f32), ((rows, width), f32), ((2 * rows, width), bf16)],
        [field, stats, peer, chip, both, c_gain, out_w, stick],
        scratch=[pltpu.VMEM((n, ch), bf16)],
        flops=2 * n * width * ch,
    )
    got = swap(send, "tp", 1).astype(f32)
    chip = swap((other + got[rows:]).astype(bf16), "tp", 2)
    return (mine + got[:rows] + chip.astype(f32)).astype(bf16)


def solution(mesh):
    return jax.shard_map(
        shards,
        mesh=mesh,
        in_specs=(
            P(("sp", "tp"), None),
            P(None, "tp"),
            P(None, "tp"),
            P(None, "tp"),
            P(None, "tp"),
            P(None, "tp"),
            P(None, "tp"),
            P("tp"),
            P("sp", "tp"),
            P("tp"),
            P("tp", None),
            P("tp", None),
        ),
        out_specs=P(("sp", "tp"), None),
        check_vma=False,
    )
```

```python
import functools

import jax
import jax.numpy as jnp
from jax import lax
from jax.experimental import pallas as pl
from jax.experimental.pallas import tpu as pltpu
from jax.sharding import PartitionSpec as P


HEAD_DIM = 128
LOG2E = 1.4426950408889634
norm_eps = 1e-05
f32 = jnp.float32
bf16 = jnp.bfloat16


def swap(value, axis, by):
    count = lax.axis_size(axis)
    return lax.ppermute(value, axis, [(i, i ^ by) for i in range(count)])


def from_behind(value, axis, by):
    count = lax.axis_size(axis)
    pairs = [(i, i + by) for i in range(count) if 0 <= i + by < count]
    return lax.ppermute(value, axis, pairs)


def dot(a, b):
    return jnp.dot(a, b, preferred_element_type=f32)


def load_kernel(*refs):
    sources, sems = refs[:12], refs[-1]
    tokens, w_in, w_gate, w_q, w_k, w_v, taps, c_gain, off, s_gain, w_c, w_s = sources
    tok, conv_w, q_w, kv_w, taps_v, c_gain_v, off_v, s_gain_v, out_w = refs[12:-1]
    ch = w_in.shape[1]
    kv = w_k.shape[1]
    pairs = [
        (w_k, kv_w.at[:, 0:kv]),
        (w_v, kv_w.at[:, kv:]),
        (w_q, q_w),
        (w_in, conv_w.at[:, 0:ch]),
        (w_gate, conv_w.at[:, ch:]),
        (tokens, tok),
        (taps, taps_v),
        (c_gain, c_gain_v),
        (off, off_v),
        (s_gain, s_gain_v),
        (w_c, out_w.at[0:ch]),
        (w_s, out_w.at[ch:]),
    ]
    copies = [pltpu.make_async_copy(a, b, sems.at[i]) for i, (a, b) in enumerate(pairs)]
    for copy in copies:
        copy.start()
    for copy in copies:
        copy.wait()


def keys_kernel(t0, t1, t2, t3, kv_w, off, pay, x_all):
    rows = t0.shape[0]
    me = lax.axis_index("tp")
    for k, t in enumerate((t0, t1, t2, t3)):
        x_all[pl.ds(pl.multiple_of((me ^ k) * rows, rows), rows), :] = t[...]
    n = x_all.shape[0]
    kv = kv_w.shape[1] // 2
    pay[0:n, :] = dot(x_all[...], kv_w[...]).astype(bf16)
    row = lax.broadcasted_iota(jnp.int32, (8, kv), 0)
    offs = off[...].astype(f32)
    head = jnp.zeros((8, kv), f32)
    for h in range(off.shape[0]):
        head = jnp.where(row == h, offs[h : h + 1, :], head)
    pay[n:, 0:kv] = head.astype(bf16)
    pay[n:, kv:] = jnp.zeros((8, kv), bf16)


def project_kernel(x_all, conv_w, q_w, pay, pay_x, qs, blend, tail):
    x = x_all[...]
    n = x.shape[0]
    ch = conv_w.shape[1] // 2
    kv = pay.shape[1] // 2
    both = dot(x, conv_w[...]).astype(bf16).astype(f32)
    q = dot(x, q_w[...]).astype(bf16)
    for h in range(q.shape[1] // HEAD_DIM):
        qs[h * n : (h + 1) * n, :] = q[:, h * HEAD_DIM : (h + 1) * HEAD_DIM]
    b = (both[:, 0:ch] * jax.nn.sigmoid(both[:, ch:])).astype(bf16)
    blend[...] = b
    tail[...] = b[n - tail.shape[0] :, :]
    pay_x[0 : n + 8, :] = pay[...]
    pay_x[n + 8 :, 0:kv] = b[n - 32 : n - 16, :]
    pay_x[n + 8 :, kv:] = b[n - 16 :, :]


def conv_kernel(even, odd, blend, taps, field, stats, wide):
    n = blend.shape[0]
    kv = odd.shape[1] // 2
    me = lax.axis_index("sp")
    right = me & 1 == 1
    for half in (0, 1):
        fill = odd[n + 8 :, half * kv : (half + 1) * kv].astype(f32)
        rest = jnp.where(me > 0, even[16 * half : 16 * half + 16, :].astype(f32), 0.0)
        wide[16 * half : 16 * half + 16, :] = jnp.where(right, fill, rest)
    convolve(blend, taps, field, stats, wide)


def conv_plain_kernel(halo, blend, taps, field, stats, wide):
    wide[0:32, :] = halo[...].astype(f32)
    convolve(blend, taps, field, stats, wide)


def convolve(blend, taps, field, stats, wide):
    n = blend.shape[0]
    reach = taps.shape[0] - 1
    wide[32 : 32 + n, :] = blend[...].astype(f32)
    base = 32 - reach
    f = taps[0:1, :] * wide[base : base + n, :]
    for t in range(1, reach + 1):
        f = f + taps[t : t + 1, :] * wide[base + t : base + t + n, :]
    field[...] = f
    ch = f.shape[1]
    mean = jnp.sum(f, axis=1, keepdims=True) / ch
    d = f - mean
    m2 = jnp.sum(d * d, axis=1, keepdims=True)
    stats[0:1, :] = jnp.transpose(jnp.broadcast_to(mean, (n, 128)))[0:1, :]
    stats[1:2, :] = jnp.transpose(jnp.broadcast_to(m2, (n, 128)))[0:1, :]


def both_stats(mean_a, m2_a, mean_b, m2_b, count):
    gap = mean_a - mean_b
    return (mean_a + mean_b) / 2, m2_a + m2_b + gap * gap * (count / 2)


def join_kernel(za, zb, joined):
    joined[0] = za[...]
    joined[1] = zb[...]


def shares(q, pays, own, n, per, tri):
    scale = LOG2E * HEAD_DIM ** (-0.5)
    takes, splits, outs = [], [], []
    for pay, mine in zip(pays, own):
        s = lax.dot_general(
            q, pay[0:n, 0:HEAD_DIM], (((1,), (1,)), ((), ())), preferred_element_type=f32
        )
        off = pay[n : n + 8, 0:HEAD_DIM].astype(f32) * LOG2E
        shift = [jnp.broadcast_to(off[h : h + 1, :], (n, n)) for h in range(per)]
        u = s * scale + jnp.concatenate(shift, axis=0)
        soft = jnp.log2(1.0 + jnp.exp2(-jnp.abs(u)))
        take = jnp.minimum(u, 0.0) - soft
        keep = take - u
        if mine:
            keep = jnp.where(before(u.shape, n), keep, 0.0)
        hi = keep.astype(bf16)
        lo = (keep - hi.astype(f32)).astype(bf16)
        takes.append(take)
        splits.append(jnp.concatenate([hi, lo], axis=1))
    for pay, mine, take, split in zip(pays, own, takes, splits):
        sums = dot(split, tri)
        w = jnp.exp2(take + sums[:, 0:n])
        if mine:
            w = jnp.where(before(w.shape, n), w, 0.0)
        outs.append((w.astype(bf16), sums[:, n : 2 * n]))
    return [
        (dot(w, pay[0:n, HEAD_DIM : 2 * HEAD_DIM]), total)
        for pay, (w, total) in zip(pays, outs)
    ]


def before(shape, n):
    row = lax.broadcasted_iota(jnp.int32, shape, 0) & (n - 1)
    return lax.broadcasted_iota(jnp.int32, shape, 1) < row


def tri_of(n):
    r = lax.broadcasted_iota(jnp.int32, (2 * n, 2 * n), 0) & (n - 1)
    c = lax.broadcasted_iota(jnp.int32, (2 * n, 2 * n), 1)
    return jnp.where((r > c) | (c >= n), 1.0, 0.0).astype(bf16)


def normed_heads(att, s_gain, mix, n, per):
    ms = jnp.mean(att * att, axis=1, keepdims=True)
    normed = att * lax.rsqrt(ms + norm_eps)
    for h in range(per):
        part = normed[h * n : (h + 1) * n, :] * s_gain[h : h + 1, :]
        mix[:, h * HEAD_DIM : (h + 1) * HEAD_DIM] = part.astype(bf16)


def by_slot(mix, n, members, slots):
    me = lax.axis_index("tp")
    rows = n // members
    picks = [mix[pl.ds(pl.multiple_of((me ^ k) * rows, rows), rows), :] for k in slots]
    return jnp.concatenate(picks, axis=0)


def parts_kernel(*refs, slots, blocks, n, per):
    q_ref = refs[0]
    pays = views(refs[1:-1])
    sums = refs[-1]
    me = lax.axis_index("sp")
    found = shares(q_ref[...], pays, [k == 0 for k in slots], n, per, tri_of(n))
    for k, (part, total) in zip(slots, found):
        j = me ^ k
        if k:
            part = jnp.where(j < me, part, 0.0)
            total = jnp.where(j < me, total, 0.0)
        sums[pl.ds(j, 1)] = part[None]
        sums[pl.ds(blocks + j, 1)] = total[None]


def views(refs):
    flat = []
    for ref in refs:
        flat += [ref] if len(ref.shape) == 2 else [ref.at[i] for i in range(ref.shape[0])]
    return flat


def stick_kernel(q_ref, *refs, slots, blocks, n, per):
    s_gain, _, mix, sums = refs[-4:]
    pays = views(refs[:-4])
    me = lax.axis_index("sp")
    late = shares(q_ref[...], pays, [False] * len(slots), n, per, tri_of(n))
    for k, (part, total) in zip(slots, late):
        j = me ^ k
        sums[pl.ds(j, 1)] = jnp.where(j < me, part, 0.0)[None]
        sums[pl.ds(blocks + j, 1)] = jnp.where(j < me, total, 0.0)[None]
    att = sums[blocks - 1]
    carry = sums[2 * blocks - 1]
    for j in range(blocks - 2, -1, -1):
        att = att + jnp.exp2(carry) * sums[j]
        if j:
            carry = carry + sums[blocks + j]
    normed_heads(att, s_gain, mix, n, per)


def stick_loop_kernel(q_ref, pays, s_gain, mix, *, n, per):
    me = lax.axis_index("sp")
    q = q_ref[...]
    tri = tri_of(n)

    def step(turn, carried):
        att, carry = carried
        ((part, total),) = shares(q, [pays.at[me - turn]], [False], n, per, tri)
        return att + jnp.exp2(carry) * part, carry + total

    (start,) = shares(q, [pays.at[me]], [True], n, per, tri)
    att, _ = lax.fori_loop(1, me + 1, step, start)
    normed_heads(att, s_gain, mix, n, per)


def send_kernel(field, own, core, chip, both, c_gain, out_w, stick, send, mix, *, members):
    n, ch = field.shape
    near = both_stats(own[0:1, :], own[1:2, :], core[0:1, :], core[1:2, :], ch)
    far = both_stats(chip[0:1, :], chip[1:2, :], both[0:1, :], both[1:2, :], ch)
    mean, m2 = both_stats(*near, *far, 2 * ch)
    rstd = lax.rsqrt(m2 / (ch * members) + norm_eps)
    mean_c = jnp.transpose(jnp.broadcast_to(mean, (ch, n)))
    rstd_c = jnp.transpose(jnp.broadcast_to(rstd, (ch, n)))
    z = (field[...] - mean_c) * rstd_c * c_gain[...]
    mix[:, 0:ch] = (z * jax.nn.sigmoid(z)).astype(bf16)
    mix[:, ch:] = stick[...]
    send[...] = dot(by_slot(mix, n, members, (1, 3)), out_w[...]).astype(bf16)


def keep_kernel(mix, out_w, mine, other, *, members):
    n = mix.shape[0]
    out = dot(by_slot(mix, n, members, (0, 2)), out_w[...])
    rows = n // members
    mine[...] = out[0:rows, :]
    other[...] = out[rows:, :]


def call(body, outs, args, scratch=(), flops=0, spaces=None, limit=2**22, aliases={}):
    in_vmem = pl.BlockSpec(memory_space=pltpu.VMEM)
    if spaces is None:
        spaces = [True] * len(args)
    args = [
        pltpu.with_memory_space_constraint(arg, pltpu.VMEM) if held else arg
        for arg, held in zip(args, spaces)
    ]
    return pl.pallas_call(
        body,
        out_shape=[pltpu.VMEM(shape, dtype) for shape, dtype in outs],
        in_specs=[in_vmem] * len(args),
        out_specs=[in_vmem] * len(outs),
        scratch_shapes=scratch,
        input_output_aliases=aliases,
        cost_estimate=pl.CostEstimate(flops=flops, transcendentals=0, bytes_accessed=0),
        compiler_params=pltpu.CompilerParams(vmem_limit_bytes=limit),
    )(*args)


def shards(
    tokens,
    conv_input,
    conv_gate,
    query_weight,
    key_weight,
    value_weight,
    conv_taps,
    conv_gain,
    key_offsets,
    stick_gain,
    conv_output,
    stick_output,
):
    members = lax.axis_size("tp")
    blocks = lax.axis_size("sp")
    rows, width = tokens.shape
    n = rows * members
    ch = conv_input.shape[1]
    kv = key_weight.shape[1]
    query_cols = query_weight.shape[1]
    per = query_cols // kv
    off = jnp.transpose(key_offsets)
    by_core = swap(tokens, "tp", 1)
    by_chip = swap(tokens, "tp", 2)
    in_vmem = pl.BlockSpec(memory_space=pltpu.VMEM)
    sources = [
        tokens, conv_input, conv_gate, query_weight, key_weight, value_weight, conv_taps,
        conv_gain.reshape(1, ch), off, stick_gain.reshape(per, HEAD_DIM),
        conv_output, stick_output,
    ]
    tok, conv_w, q_w, kv_w, taps, c_gain, off, s_gain, out_w = pl.pallas_call(
        load_kernel,
        out_shape=[
            pltpu.VMEM(shape, dtype)
            for shape, dtype in (
                ((rows, width), bf16),
                ((width, 2 * ch), bf16),
                ((width, query_cols), bf16),
                ((width, 2 * kv), bf16),
                (conv_taps.shape, f32),
                ((1, ch), f32),
                ((per, n), bf16),
                ((per, HEAD_DIM), f32),
                ((ch + query_cols, width), bf16),
            )
        ],
        in_specs=[pl.BlockSpec(memory_space=pltpu.HBM)] * 12,
        out_specs=[in_vmem] * 9,
        scratch_shapes=[pltpu.SemaphoreType.DMA((12,))],
        cost_estimate=pl.CostEstimate(flops=10**9, transcendentals=0, bytes_accessed=5 * 10**6),
        compiler_params=pltpu.CompilerParams(vmem_limit_bytes=2**21),
    )(*[pltpu.with_memory_space_constraint(source, pltpu.HBM) for source in sources])
    by_chip, tok = lax.optimization_barrier((by_chip, tok))
    by_both = swap(by_chip, "tp", 1)
    pay, x_all = call(
        keys_kernel,
        [((n + 8, 2 * kv), bf16), ((n, width), bf16)],
        [tok, by_core, by_chip, by_both, kv_w, off],
        flops=2 * n * width * 2 * kv,
    )
    pay_x, qs, blend, tail = call(
        project_kernel,
        [
            ((n + 24, 2 * kv), bf16),
            ((per * n, HEAD_DIM), bf16),
            ((n, ch), bf16),
            ((32, ch), bf16),
        ],
        [x_all, conv_w, q_w, pay],
        flops=2 * n * width * (2 * ch + query_cols),
    )
    sizes = dict(n=n, per=per)
    heads = per * n
    block_flops = 2 * heads * n * HEAD_DIM * 8
    stat = ((8, n), f32)
    if blocks == 8:
        z2 = swap(pay, "sp", 2)
        z6 = swap(pay, "sp", 6)
        z4 = swap(pay, "sp", 4)
        x1 = swap(pay_x, "sp", 1)
        x3 = swap(z2, "sp", 1)
        pairs = []
        for i in range(1, blocks - 1, 2):
            pairs += [(i, i + 1), (i + 1, i)]
        even = lax.ppermute(tail, "sp", pairs)
        conv_body = conv_kernel
        conv_args = [even, x1, blend, taps]
    else:
        pays = lax.all_gather(pay, "sp", axis=0)
        conv_body = conv_plain_kernel
        conv_args = [from_behind(tail, "sp", 1), blend, taps]
    field, stats = call(
        conv_body,
        [((n, ch), f32), stat],
        conv_args,
        [pltpu.VMEM((n + 32, ch), f32)],
        64 * n * ch,
    )
    peer = swap(stats, "tp", 1)
    chip = swap(stats, "tp", 2)
    both = swap(stats, "tp", 3)
    if blocks == 8:
        (z46,) = call(join_kernel, [((2, n + 8, 2 * kv), bf16)], [z4, z6])
        x57 = swap(z46, "sp", 1)
        (sums,) = call(
            functools.partial(parts_kernel, slots=(0, 2, 1, 3, 4, 6), blocks=blocks, **sizes),
            [((2 * blocks, heads, HEAD_DIM), f32)],
            [qs, pay, z2, x1, x3, z46],
            flops=6 * block_flops,
        )
        body = functools.partial(
            stick_kernel, slots=(5, 7), blocks=blocks, **sizes
        )
        stick_args = [qs, x57, s_gain, sums]
        stick_outs = [((2 * blocks, heads, HEAD_DIM), f32)]
        aliases = {3: 1}
        spaces = None
    else:
        body = functools.partial(stick_loop_kernel, **sizes)
        stick_args = [qs, pays, s_gain]
        stick_outs = []
        aliases = {}
        spaces = [True, False, True]
    stick, *_ = call(
        body,
        [((n, query_cols), bf16)] + stick_outs,
        stick_args,
        flops=block_flops,
        spaces=spaces,
        aliases=aliases,
        limit=2**22 if blocks == 8 else 2**25,
    )
    send, mix = call(
        functools.partial(send_kernel, members=members),
        [((2 * rows, width), bf16), ((n, ch + query_cols), bf16)],
        [field, stats, peer, chip, both, c_gain, out_w, stick],
        flops=n * width * (ch + query_cols),
    )
    mine, other = call(
        functools.partial(keep_kernel, members=members),
        [((rows, width), f32), ((rows, width), f32)],
        [mix, out_w],
        flops=n * width * (ch + query_cols),
    )
    got = swap(send, "tp", 1).astype(f32)
    chip = swap((other + got[rows:]).astype(bf16), "tp", 2)
    return (mine + got[:rows] + chip.astype(f32)).astype(bf16)


def solution(mesh):
    return jax.shard_map(
        shards,
        mesh=mesh,
        in_specs=(
            P(("sp", "tp"), None),
            P(None, "tp"),
            P(None, "tp"),
            P(None, "tp"),
            P(None, "tp"),
            P(None, "tp"),
            P(None, "tp"),
            P("tp"),
            P("sp", "tp"),
            P("tp"),
            P("tp", None),
            P("tp", None),
        ),
        out_specs=P(("sp", "tp"), None),
        check_vma=False,
    )
```

```python
import functools

import jax
import jax.numpy as jnp
from jax import lax
from jax.experimental import pallas as pl
from jax.experimental.pallas import tpu as pltpu
from jax.sharding import PartitionSpec as P


HEAD_DIM = 128
LOG2E = 1.4426950408889634
norm_eps = 1e-05
f32 = jnp.float32
bf16 = jnp.bfloat16


def swap(value, axis, by):
    count = lax.axis_size(axis)
    return lax.ppermute(value, axis, [(i, i ^ by) for i in range(count)])


def from_behind(value, axis, by):
    count = lax.axis_size(axis)
    pairs = [(i, i + by) for i in range(count) if 0 <= i + by < count]
    return lax.ppermute(value, axis, pairs)


def dot(a, b):
    return jnp.dot(a, b, preferred_element_type=f32)


def load_kernel(*refs):
    sources, sems = refs[:12], refs[-1]
    tokens, w_in, w_gate, w_q, w_k, w_v, taps, c_gain, off, s_gain, w_c, w_s = sources
    tok, conv_w, q_w, kv_w, taps_v, c_gain_v, off_v, s_gain_v, out_w = refs[12:-1]
    ch = w_in.shape[1]
    kv = w_k.shape[1]
    pairs = [
        (w_k, kv_w.at[:, 0:kv]),
        (w_v, kv_w.at[:, kv:]),
        (w_q, q_w),
        (w_in, conv_w.at[:, 0:ch]),
        (w_gate, conv_w.at[:, ch:]),
        (tokens, tok),
        (taps, taps_v),
        (c_gain, c_gain_v),
        (off, off_v),
        (s_gain, s_gain_v),
        (w_c, out_w.at[0:ch]),
        (w_s, out_w.at[ch:]),
    ]
    copies = [pltpu.make_async_copy(a, b, sems.at[i]) for i, (a, b) in enumerate(pairs)]
    for copy in copies:
        copy.start()
    for copy in copies:
        copy.wait()


def keys_kernel(t0, t1, t2, t3, kv_w, off, pay, x_all):
    rows = t0.shape[0]
    me = lax.axis_index("tp")
    for k, t in enumerate((t0, t1, t2, t3)):
        x_all[pl.ds(pl.multiple_of((me ^ k) * rows, rows), rows), :] = t[...]
    n = x_all.shape[0]
    kv = kv_w.shape[1] // 2
    pay[0:n, :] = dot(x_all[...], kv_w[...]).astype(bf16)
    row = lax.broadcasted_iota(jnp.int32, (8, kv), 0)
    offs = off[...].astype(f32)
    head = jnp.zeros((8, kv), f32)
    for h in range(off.shape[0]):
        head = jnp.where(row == h, offs[h : h + 1, :], head)
    pay[n:, 0:kv] = head.astype(bf16)
    pay[n:, kv:] = jnp.zeros((8, kv), bf16)


def project_kernel(x_all, conv_w, q_w, pay, pay_x, qs, blend, tail):
    x = x_all[...]
    n = x.shape[0]
    ch = conv_w.shape[1] // 2
    kv = pay.shape[1] // 2
    both = dot(x, conv_w[...]).astype(bf16).astype(f32)
    q = dot(x, q_w[...]).astype(bf16)
    for h in range(q.shape[1] // HEAD_DIM):
        qs[h * n : (h + 1) * n, :] = q[:, h * HEAD_DIM : (h + 1) * HEAD_DIM]
    b = (both[:, 0:ch] * jax.nn.sigmoid(both[:, ch:])).astype(bf16)
    blend[...] = b
    tail[...] = b[n - tail.shape[0] :, :]
    pay_x[0 : n + 8, :] = pay[...]
    pay_x[n + 8 :, 0:kv] = b[n - 32 : n - 16, :]
    pay_x[n + 8 :, kv:] = b[n - 16 :, :]


def conv_kernel(even, odd, blend, taps, field, stats, wide):
    n = blend.shape[0]
    kv = odd.shape[1] // 2
    me = lax.axis_index("sp")
    right = me & 1 == 1
    for half in (0, 1):
        fill = odd[n + 8 :, half * kv : (half + 1) * kv].astype(f32)
        rest = jnp.where(me > 0, even[16 * half : 16 * half + 16, :].astype(f32), 0.0)
        wide[16 * half : 16 * half + 16, :] = jnp.where(right, fill, rest)
    convolve(blend, taps, field, stats, wide)


def conv_plain_kernel(halo, blend, taps, field, stats, wide):
    wide[0:32, :] = halo[...].astype(f32)
    convolve(blend, taps, field, stats, wide)


def convolve(blend, taps, field, stats, wide):
    n = blend.shape[0]
    reach = taps.shape[0] - 1
    wide[32 : 32 + n, :] = blend[...].astype(f32)
    base = 32 - reach
    f = taps[0:1, :] * wide[base : base + n, :]
    for t in range(1, reach + 1):
        f = f + taps[t : t + 1, :] * wide[base + t : base + t + n, :]
    field[...] = f
    ch = f.shape[1]
    mean = jnp.sum(f, axis=1, keepdims=True) / ch
    d = f - mean
    m2 = jnp.sum(d * d, axis=1, keepdims=True)
    stats[0:1, :] = jnp.transpose(jnp.broadcast_to(mean, (n, 128)))[0:1, :]
    stats[1:2, :] = jnp.transpose(jnp.broadcast_to(m2, (n, 128)))[0:1, :]


def both_stats(mean_a, m2_a, mean_b, m2_b, count):
    gap = mean_a - mean_b
    return (mean_a + mean_b) / 2, m2_a + m2_b + gap * gap * (count / 2)


def join_kernel(za, zb, joined):
    joined[0] = za[...]
    joined[1] = zb[...]


def shares(q, pays, own, n, per, tri):
    scale = LOG2E * HEAD_DIM ** (-0.5)
    takes, splits, outs = [], [], []
    for pay, mine in zip(pays, own):
        s = lax.dot_general(
            q, pay[0:n, 0:HEAD_DIM], (((1,), (1,)), ((), ())), preferred_element_type=f32
        )
        off = pay[n : n + 8, 0:HEAD_DIM].astype(f32) * LOG2E
        shift = [jnp.broadcast_to(off[h : h + 1, :], (n, n)) for h in range(per)]
        u = s * scale + jnp.concatenate(shift, axis=0)
        soft = jnp.log2(1.0 + jnp.exp2(-jnp.abs(u)))
        take = jnp.minimum(u, 0.0) - soft
        keep = jnp.minimum(-u, 0.0) - soft
        if mine:
            keep = jnp.where(before(u.shape, n), keep, 0.0)
        hi = keep.astype(bf16)
        lo = (keep - hi.astype(f32)).astype(bf16)
        takes.append(take)
        splits.append(jnp.concatenate([hi, lo], axis=1))
    for pay, mine, take, split in zip(pays, own, takes, splits):
        sums = dot(split, tri)
        w = jnp.exp2(take + sums[:, 0:n])
        if mine:
            w = jnp.where(before(w.shape, n), w, 0.0)
        outs.append((w.astype(bf16), sums[:, n : 2 * n]))
    return [
        (dot(w, pay[0:n, HEAD_DIM : 2 * HEAD_DIM]), total)
        for pay, (w, total) in zip(pays, outs)
    ]


def before(shape, n):
    row = lax.broadcasted_iota(jnp.int32, shape, 0) & (n - 1)
    return lax.broadcasted_iota(jnp.int32, shape, 1) < row


def tri_of(n):
    r = lax.broadcasted_iota(jnp.int32, (2 * n, 2 * n), 0) & (n - 1)
    c = lax.broadcasted_iota(jnp.int32, (2 * n, 2 * n), 1)
    return jnp.where((r > c) | (c >= n), 1.0, 0.0).astype(bf16)


def normed_heads(att, s_gain, mix, n, per):
    ms = jnp.mean(att * att, axis=1, keepdims=True)
    normed = att * lax.rsqrt(ms + norm_eps)
    for h in range(per):
        part = normed[h * n : (h + 1) * n, :] * s_gain[h : h + 1, :]
        mix[:, h * HEAD_DIM : (h + 1) * HEAD_DIM] = part.astype(bf16)


def by_slot(mix, n, members, slots):
    me = lax.axis_index("tp")
    rows = n // members
    picks = [mix[pl.ds(pl.multiple_of((me ^ k) * rows, rows), rows), :] for k in slots]
    return jnp.concatenate(picks, axis=0)


def parts_kernel(*refs, slots, blocks, n, per):
    q_ref = refs[0]
    pays = views(refs[1:-1])
    sums = refs[-1]
    me = lax.axis_index("sp")
    found = shares(q_ref[...], pays, [k == 0 for k in slots], n, per, tri_of(n))
    for k, (part, total) in zip(slots, found):
        j = me ^ k
        if k:
            part = jnp.where(j < me, part, 0.0)
            total = jnp.where(j < me, total, 0.0)
        sums[pl.ds(j, 1)] = part[None]
        sums[pl.ds(blocks + j, 1)] = total[None]


def views(refs):
    flat = []
    for ref in refs:
        flat += [ref] if len(ref.shape) == 2 else [ref.at[i] for i in range(ref.shape[0])]
    return flat


def stick_kernel(q_ref, *refs, slots, blocks, n, per):
    s_gain, _, mix, sums = refs[-4:]
    pays = views(refs[:-4])
    me = lax.axis_index("sp")
    late = shares(q_ref[...], pays, [False] * len(slots), n, per, tri_of(n))
    for k, (part, total) in zip(slots, late):
        j = me ^ k
        sums[pl.ds(j, 1)] = jnp.where(j < me, part, 0.0)[None]
        sums[pl.ds(blocks + j, 1)] = jnp.where(j < me, total, 0.0)[None]
    att = sums[blocks - 1]
    carry = sums[2 * blocks - 1]
    for j in range(blocks - 2, -1, -1):
        att = att + jnp.exp2(carry) * sums[j]
        if j:
            carry = carry + sums[blocks + j]
    normed_heads(att, s_gain, mix, n, per)


def stick_loop_kernel(q_ref, pays, s_gain, mix, *, n, per):
    me = lax.axis_index("sp")
    q = q_ref[...]
    tri = tri_of(n)

    def step(turn, carried):
        att, carry = carried
        ((part, total),) = shares(q, [pays.at[me - turn]], [False], n, per, tri)
        return att + jnp.exp2(carry) * part, carry + total

    (start,) = shares(q, [pays.at[me]], [True], n, per, tri)
    att, _ = lax.fori_loop(1, me + 1, step, start)
    normed_heads(att, s_gain, mix, n, per)


def send_kernel(field, own, core, chip, both, c_gain, out_w, stick, send, mix, *, members):
    n, ch = field.shape
    near = both_stats(own[0:1, :], own[1:2, :], core[0:1, :], core[1:2, :], ch)
    far = both_stats(chip[0:1, :], chip[1:2, :], both[0:1, :], both[1:2, :], ch)
    mean, m2 = both_stats(*near, *far, 2 * ch)
    rstd = lax.rsqrt(m2 / (ch * members) + norm_eps)
    mean_c = jnp.transpose(jnp.broadcast_to(mean, (ch, n)))
    rstd_c = jnp.transpose(jnp.broadcast_to(rstd, (ch, n)))
    z = (field[...] - mean_c) * rstd_c * c_gain[...]
    mix[:, 0:ch] = (z * jax.nn.sigmoid(z)).astype(bf16)
    mix[:, ch:] = stick[...]
    send[...] = dot(by_slot(mix, n, members, (1, 3)), out_w[...]).astype(bf16)


def keep_kernel(mix, out_w, mine, other, *, members):
    n = mix.shape[0]
    out = dot(by_slot(mix, n, members, (0, 2)), out_w[...])
    rows = n // members
    mine[...] = out[0:rows, :]
    other[...] = out[rows:, :]


def call(body, outs, args, scratch=(), flops=0, spaces=None, limit=2**22, aliases={}):
    in_vmem = pl.BlockSpec(memory_space=pltpu.VMEM)
    if spaces is None:
        spaces = [True] * len(args)
    args = [
        pltpu.with_memory_space_constraint(arg, pltpu.VMEM) if held else arg
        for arg, held in zip(args, spaces)
    ]
    return pl.pallas_call(
        body,
        out_shape=[pltpu.VMEM(shape, dtype) for shape, dtype in outs],
        in_specs=[in_vmem] * len(args),
        out_specs=[in_vmem] * len(outs),
        scratch_shapes=scratch,
        input_output_aliases=aliases,
        cost_estimate=pl.CostEstimate(flops=flops, transcendentals=0, bytes_accessed=0),
        compiler_params=pltpu.CompilerParams(vmem_limit_bytes=limit),
    )(*args)


def shards(
    tokens,
    conv_input,
    conv_gate,
    query_weight,
    key_weight,
    value_weight,
    conv_taps,
    conv_gain,
    key_offsets,
    stick_gain,
    conv_output,
    stick_output,
):
    members = lax.axis_size("tp")
    blocks = lax.axis_size("sp")
    rows, width = tokens.shape
    n = rows * members
    ch = conv_input.shape[1]
    kv = key_weight.shape[1]
    query_cols = query_weight.shape[1]
    per = query_cols // kv
    off = jnp.transpose(key_offsets)
    by_core = swap(tokens, "tp", 1)
    by_chip = swap(tokens, "tp", 2)
    in_vmem = pl.BlockSpec(memory_space=pltpu.VMEM)
    sources = [
        tokens, conv_input, conv_gate, query_weight, key_weight, value_weight, conv_taps,
        conv_gain.reshape(1, ch), off, stick_gain.reshape(per, HEAD_DIM),
        conv_output, stick_output,
    ]
    tok, conv_w, q_w, kv_w, taps, c_gain, off, s_gain, out_w = pl.pallas_call(
        load_kernel,
        out_shape=[
            pltpu.VMEM(shape, dtype)
            for shape, dtype in (
                ((rows, width), bf16),
                ((width, 2 * ch), bf16),
                ((width, query_cols), bf16),
                ((width, 2 * kv), bf16),
                (conv_taps.shape, f32),
                ((1, ch), f32),
                ((per, n), bf16),
                ((per, HEAD_DIM), f32),
                ((ch + query_cols, width), bf16),
            )
        ],
        in_specs=[pl.BlockSpec(memory_space=pltpu.HBM)] * 12,
        out_specs=[in_vmem] * 9,
        scratch_shapes=[pltpu.SemaphoreType.DMA((12,))],
        cost_estimate=pl.CostEstimate(flops=10**9, transcendentals=0, bytes_accessed=5 * 10**6),
        compiler_params=pltpu.CompilerParams(vmem_limit_bytes=2**21),
    )(*[pltpu.with_memory_space_constraint(source, pltpu.HBM) for source in sources])
    by_chip, tok = lax.optimization_barrier((by_chip, tok))
    by_both = swap(by_chip, "tp", 1)
    pay, x_all = call(
        keys_kernel,
        [((n + 8, 2 * kv), bf16), ((n, width), bf16)],
        [tok, by_core, by_chip, by_both, kv_w, off],
        flops=2 * n * width * 2 * kv,
    )
    pay_x, qs, blend, tail = call(
        project_kernel,
        [
            ((n + 24, 2 * kv), bf16),
            ((per * n, HEAD_DIM), bf16),
            ((n, ch), bf16),
            ((32, ch), bf16),
        ],
        [x_all, conv_w, q_w, pay],
        flops=2 * n * width * (2 * ch + query_cols),
    )
    sizes = dict(n=n, per=per)
    heads = per * n
    block_flops = 2 * heads * n * HEAD_DIM * 8
    stat = ((8, n), f32)
    if blocks == 8:
        z2 = swap(pay, "sp", 2)
        z6 = swap(pay, "sp", 6)
        z4 = swap(pay, "sp", 4)
        x1 = swap(pay_x, "sp", 1)
        x3 = swap(z2, "sp", 1)
        pairs = []
        for i in range(1, blocks - 1, 2):
            pairs += [(i, i + 1), (i + 1, i)]
        even = lax.ppermute(tail, "sp", pairs)
        conv_body = conv_kernel
        conv_args = [even, x1, blend, taps]
    else:
        pays = lax.all_gather(pay, "sp", axis=0)
        conv_body = conv_plain_kernel
        conv_args = [from_behind(tail, "sp", 1), blend, taps]
    field, stats = call(
        conv_body,
        [((n, ch), f32), stat],
        conv_args,
        [pltpu.VMEM((n + 32, ch), f32)],
        64 * n * ch,
    )
    peer = swap(stats, "tp", 1)
    chip = swap(stats, "tp", 2)
    both = swap(stats, "tp", 3)
    if blocks == 8:
        (z46,) = call(join_kernel, [((2, n + 8, 2 * kv), bf16)], [z4, z6])
        x57 = swap(z46, "sp", 1)
        (sums,) = call(
            functools.partial(parts_kernel, slots=(0, 2, 1, 3, 4, 6), blocks=blocks, **sizes),
            [((2 * blocks, heads, HEAD_DIM), f32)],
            [qs, pay, z2, x1, x3, z46],
            flops=6 * block_flops,
        )
        body = functools.partial(
            stick_kernel, slots=(5, 7), blocks=blocks, **sizes
        )
        stick_args = [qs, x57, s_gain, sums]
        stick_outs = [((2 * blocks, heads, HEAD_DIM), f32)]
        aliases = {3: 1}
        spaces = None
    else:
        body = functools.partial(stick_loop_kernel, **sizes)
        stick_args = [qs, pays, s_gain]
        stick_outs = []
        aliases = {}
        spaces = [True, False, True]
    stick, *_ = call(
        body,
        [((n, query_cols), bf16)] + stick_outs,
        stick_args,
        flops=block_flops,
        spaces=spaces,
        aliases=aliases,
        limit=2**22 if blocks == 8 else 2**25,
    )
    send, mix = call(
        functools.partial(send_kernel, members=members),
        [((2 * rows, width), bf16), ((n, ch + query_cols), bf16)],
        [field, stats, peer, chip, both, c_gain, out_w, stick],
        flops=n * width * (ch + query_cols),
    )
    mine, other = call(
        functools.partial(keep_kernel, members=members),
        [((rows, width), f32), ((rows, width), f32)],
        [mix, out_w],
        flops=n * width * (ch + query_cols),
    )
    got = swap(send, "tp", 1)
    chip = swap((other + got[rows:].astype(f32)).astype(bf16), "tp", 2)
    return (mine + got[:rows].astype(f32) + chip.astype(f32)).astype(bf16)


def solution(mesh):
    return jax.shard_map(
        shards,
        mesh=mesh,
        in_specs=(
            P(("sp", "tp"), None),
            P(None, "tp"),
            P(None, "tp"),
            P(None, "tp"),
            P(None, "tp"),
            P(None, "tp"),
            P(None, "tp"),
            P("tp"),
            P("sp", "tp"),
            P("tp"),
            P("tp", None),
            P("tp", None),
        ),
        out_specs=P(("sp", "tp"), None),
        check_vma=False,
    )
```
